32 devices in a mesh: sp: 8 (over z, y), tp: 4 (over x, core).
Axes of the slice: x: 2, y: 2, z: 4, core: 2. Of those that a mesh axis runs over, the one named last changes fastest.
Arguments:
- stream: bfloat16 [1024, 2048], P('sp'), may hold values from -12 to 12
- out_grad: bfloat16 [1024, 2048], P('sp'), may hold values from -6 to 6
- routes: int32 [1024, 2], P('sp'), may hold values from 0 to 7, all different within a row; in each aligned block of 128 rows (0 to 127, 128 to 255, ...) at most 64 rows name the same one
- route_weight: float32 [1024, 2], P('sp'), may hold values from 0.2 to 1
- queries: bfloat16 [1024, 8, 128], P('sp', 'tp'), may hold values from -6 to 6
- key_vectors: bfloat16 [1024, 8, 128], P('sp', 'tp'), may hold values from -6 to 6
- value_vectors: bfloat16 [1024, 8, 256], P('sp', 'tp'), may hold values from -6 to 6
- log_decay: float32 [1024, 8], P('sp', 'tp'), may hold values from -1 to 0
- out_proj: bfloat16 [2048, 2048], P(None, 'tp'), may hold values from -0.125 to 0.125
- gate_weight: bfloat16 [8, 2048, 1024], P('sp', None, 'tp'), may hold values from -0.125 to 0.125
- up_weight: bfloat16 [8, 2048, 1024], P('sp', None, 'tp'), may hold values from -0.125 to 0.125
- down_weight: bfloat16 [8, 1024, 2048], P('sp', 'tp'), may hold values from -0.1875 to 0.1875
Outputs:
- gate_grad: bfloat16 [8, 2048, 1024], P('sp', None, 'tp')
- up_grad: bfloat16 [8, 2048, 1024], P('sp', None, 'tp')
- down_grad: bfloat16 [8, 1024, 2048], P('sp', 'tp')
- proj_grad: float32 [2048, 2048], P('sp', 'tp')
- query_grad: bfloat16 [1024, 8, 128], P('sp', 'tp')
- key_grad: bfloat16 [1024, 8, 128], P('sp', 'tp')
- value_grad: bfloat16 [1024, 8, 256], P('sp', 'tp')
The draws below stay inside these ranges and needn't reach their ends.
Inputs may be any that keep to these rules, and one draw needn't show every extreme that they name: `routes`: each row names two different experts. In each aligned block of 128 rows no expert is named by more than 64 rows, and in some block an expert is named by exactly 64.
All inputs are finite; a program needn't handle non-finite values.
Results may differ from the reference program's by a relative error of at most 0.025.
Values may be sent and summed in bfloat16 or wider, within the bound.
A program may use at most 128 MiB of HBM per device.

```python
import math
import jax
import jax.numpy as jnp
import numpy as np
from jax import lax

D = 2048
RETENTION_HEADS = 8
KD = 128
VD = 256
FF = 1024
TOK_DEV = 128
SEQUENCE_TOKENS = 1024
EXPERTS = 8
CAP = 64
HV = 2048
N_SP = 8
N_TP = 4


def draw_log_decay(key, part):
    random_subkeys = jax.random.split(jax.random.fold_in(key, 7), 7)
    ranking = jax.random.permutation(random_subkeys[0], RETENTION_HEADS)
    slow_rate = jax.random.uniform(random_subkeys[1], (RETENTION_HEADS,), jnp.float32, 0.05, 0.2) / SEQUENCE_TOKENS
    fast_rate = jnp.exp(jax.random.uniform(random_subkeys[2], (RETENTION_HEADS,), jnp.float32, math.log(0.012), math.log(0.025)))
    baseline_decay_rate = jnp.where(ranking < RETENTION_HEADS // 2, fast_rate, slow_rate)
    decay_factor = jnp.exp(jax.random.uniform(random_subkeys[3], (SEQUENCE_TOKENS // TOK_DEV, RETENTION_HEADS), jnp.float32, 0.0, math.log(3.0)))
    decay_factor = jnp.repeat(decay_factor, TOK_DEV, axis=0)
    jitter_amount = jax.random.uniform(random_subkeys[4], (SEQUENCE_TOKENS, RETENTION_HEADS), jnp.float32, 0.6, 1.4)
    spike_location = jax.random.randint(random_subkeys[5], (2, RETENTION_HEADS), 0, SEQUENCE_TOKENS)
    spike_depth = jax.random.uniform(random_subkeys[6], (2, RETENTION_HEADS), jnp.float32, math.log(0.5), math.log(0.8))
    token_position = jnp.arange(SEQUENCE_TOKENS, dtype=jnp.int32)[:, None]
    spike_events = jnp.where(token_position == spike_location[0][None, :], spike_depth[0][None, :], 0.0)
    spike_events = spike_events + jnp.where(token_position == spike_location[1][None, :], spike_depth[1][None, :], 0.0)
    return -(baseline_decay_rate[None, :] * decay_factor * jitter_amount) + spike_events


def strengthened(drawn, own_key, source, target, shards_of, factor):
    def block_of(position):
        return (jnp.arange(drawn.shape[position]) // (drawn.shape[position] // shards_of)).reshape((-1,) + (1,) * (drawn.ndim - 1 - position))

    first = jax.random.permutation(own_key, shards_of)[block_of(target)]
    far = (block_of(target) + shards_of // 2) % shards_of
    return jnp.where((block_of(source) == first) | (block_of(source) == far), factor * drawn, drawn)


def block_levels(rng, extent, cuts, least, largest):
    loudness, own = 1.0, jax.random.fold_in(rng, 6)
    for position, blocks in cuts:
        draws = jnp.exp(jax.random.uniform(jax.random.fold_in(own, position), (blocks,), jnp.float32, least / len(cuts), largest / len(cuts)))
        loudness = loudness * jnp.repeat(draws, extent[position] // blocks).reshape([-1 if axis == position else 1 for axis in range(len(extent))])
    return loudness


def deal_out(own_key, own, number, rows, count, top, reach, skew):
    sequence = jax.random.permutation(own_key, count)
    heavy_load, common = portions_of(count, rows * top, reach, skew, True), portions_of(count, rows * top, reach, skew, False)
    places = jnp.arange(count)

    def named(sizes, rotation):
        used = int((sizes > 0).sum())
        fixed = max(1, used // 4)
        moved = fixed + (places - fixed + rotation * (used - fixed)) % max(1, count - fixed)
        return jnp.zeros((count,), jnp.int32).at[sequence[jnp.where(places < fixed, places, moved)]].set(jnp.asarray(sizes, jnp.int32))

    sizes = jnp.where(number % 4 == 0, named(heavy_load, number // 4), named(common, number - number // 4 - 1))
    mixed = jax.random.permutation(jax.random.fold_in(own, 3), count)
    donor, taker = mixed[0:count // 2 * 2:2], mixed[1:count // 2 * 2:2]
    slack = jnp.minimum(sizes[donor] - 1, reach - sizes[taker]) // 2
    slack = jnp.where((donor == sequence[0]) | (taker == sequence[0]) | (sizes[taker] == 0), 0, jnp.maximum(slack, 0))
    moved = jax.random.randint(jax.random.fold_in(own, 4), (count // 2,), 0, 1 << 20) % (slack + 1)
    sizes = sizes.at[donor].add(-moved).at[taker].add(moved)
    members = jnp.searchsorted(jnp.cumsum(sizes), jnp.arange(rows * top), side="right").astype(jnp.int32)
    listing = members.reshape(top, rows).T
    listing = listing[jax.random.permutation(jax.random.fold_in(own, 1), rows)]
    rotation = jax.random.randint(jax.random.fold_in(own, 2), (rows, 1), 0, top)
    return jnp.take_along_axis(listing, (jnp.arange(top)[None, :] + rotation) % top, axis=1)


def portions_of(number_of, total, most, skew, full):
    loads = [(1 << 20) // math.isqrt(standing ** skew) + 1 for standing in range(1, number_of + 1)]
    largest = most if full else min(most, max(-(-total // number_of), total * loads[0] // sum(loads)))
    least = 1 if total - largest >= number_of - 1 else 0
    given, spare = [largest] + [least] * (number_of - 1), total - largest - least * (number_of - 1)
    while spare > 0:
        movable = [i for i in range(1, number_of) if given[i] < largest] or [i for i in range(1, number_of) if given[i] < most]
        pool, remaining = sum([loads[i] for i in movable]), spare
        for i in movable:
            more = min(most - given[i], max(1, remaining * loads[i] // pool), spare)
            given[i] = given[i] + more
            spare = spare - more
    return np.array(given)


def bell_draw(own_key, extent, scale, limit, cuts=(), kind=jnp.bfloat16):
    level = block_levels(own_key, extent, cuts, -0.22, 0.18) if cuts else 1.0
    values = jax.random.normal(own_key, extent, jnp.float32) * scale * level
    return jnp.minimum(jnp.maximum(values, -limit), limit).astype(kind)


def gaussian_with(stream_key, shape, width, limit, cuts, heavy, kind=jnp.bfloat16):
    result = width * jax.random.normal(stream_key, shape, jnp.float32)
    if cuts:
        result = result * block_levels(stream_key, shape, cuts, -0.22, 0.18)
    return jnp.clip(strengthened(result, jax.random.fold_in(stream_key, 3), *heavy), -limit, limit).astype(kind)


def setup_inputs(seed: int = 0) -> dict:
    arg_keys = jax.random.split(jax.random.key(seed), 13)
    stream = bell_draw(arg_keys[0], (SEQUENCE_TOKENS, D), 2.5, 12.0, ((0, 8),))
    out_grad = gaussian_with(arg_keys[1], (SEQUENCE_TOKENS, D), 1.0, 6.0, ((0, 8),), (0, 1, 8, 2.0))
    routes_keys = jax.random.split(jax.random.fold_in(arg_keys[2], 1), SEQUENCE_TOKENS // TOK_DEV)
    routes_turns = jax.random.permutation(jax.random.fold_in(arg_keys[2], 3), SEQUENCE_TOKENS // TOK_DEV)
    routes = jax.vmap(lambda own, number: deal_out(jax.random.fold_in(arg_keys[2], 2), own, number, TOK_DEV, EXPERTS, 2, CAP, 1))(routes_keys, routes_turns).reshape((SEQUENCE_TOKENS, 2))
    route_weight = jnp.clip(jnp.exp(math.log(1.0) - 1.609438 * jax.random.uniform(arg_keys[3], (SEQUENCE_TOKENS, 2), jnp.float32) ** block_levels(arg_keys[3], (SEQUENCE_TOKENS, 2), ((0, 8),), -0.2, 0.2)), 0.2, 1.0)
    queries = bell_draw(arg_keys[4], (SEQUENCE_TOKENS, RETENTION_HEADS, KD), 1.0, 6.0, ((0, 8), (1, 4)))
    key_vectors = bell_draw(arg_keys[5], (SEQUENCE_TOKENS, RETENTION_HEADS, KD), 1.0, 6.0, ((0, 8), (1, 4)))
    value_vectors = bell_draw(arg_keys[6], (SEQUENCE_TOKENS, RETENTION_HEADS, VD), 1.0, 6.0, ((0, 8), (1, 4)))
    log_decay = draw_log_decay(jax.random.fold_in(arg_keys[12], 71), 0)
    out_proj = bell_draw(arg_keys[8], (D, HV), HV ** -0.5, 0.125, ((1, 4),))
    gate_weight = bell_draw(arg_keys[9], (EXPERTS, D, FF), D ** -0.5, 0.125, ((0, 8), (2, 4)))
    up_weight = bell_draw(arg_keys[10], (EXPERTS, D, FF), D ** -0.5, 0.125, ((0, 8), (2, 4)))
    down_weight = bell_draw(arg_keys[11], (EXPERTS, FF, D), FF ** -0.5, 0.1875, ((0, 8), (1, 4)))
    return dict(stream=stream, out_grad=out_grad, routes=routes, route_weight=route_weight, queries=queries, key_vectors=key_vectors, value_vectors=value_vectors, log_decay=log_decay, out_proj=out_proj, gate_weight=gate_weight, up_weight=up_weight, down_weight=down_weight)


CLAMP_LIMIT = 7.0
GATE_SLOPE = 1.702
EPSILON = 1e-06
TOP_PRECISION = lax.Precision.HIGHEST

def slot_numbers(route_block, expert_count):
    flat_ids = route_block.reshape(-1)
    onehot = (flat_ids[:, None] == jnp.arange(expert_count, dtype=jnp.int32)[None, :]).astype(jnp.int32)
    before = jnp.cumsum(onehot, axis=0) - onehot
    return (flat_ids, lax.optimization_barrier(jnp.sum(before * onehot, axis=1)).astype(jnp.int32))

def rotation_tables(start, count, key_width):
    frequency = 1.0 / 10000.0 ** jnp.linspace(0.0, 1.0, key_width // 2, dtype=jnp.float32)
    token_position = (start + jnp.arange(count, dtype=jnp.int32)).astype(jnp.float32)
    angles = token_position[:, None] * frequency[None, :]
    return (jnp.cos(angles), jnp.sin(angles))

def turn(field, cosines, sines):
    paired = field.reshape(field.shape[:-1] + (field.shape[-1] // 2, 2))
    even_part = paired[..., 0]
    odd_part = paired[..., 1]
    cos_rows = cosines[:, None, :]
    sin_rows = sines[:, None, :]
    turned = jnp.stack([even_part * cos_rows - odd_part * sin_rows, odd_part * cos_rows + even_part * sin_rows], axis=-1)
    return turned.reshape(field.shape)

def expert_pass(routed_rows, routed_grads, gate_w, up_w, down_w):
    gate_pre = jnp.dot(routed_rows, gate_w, preferred_element_type=jnp.float32)
    up_pre = jnp.dot(routed_rows, up_w, preferred_element_type=jnp.float32)
    gate_clip = jnp.minimum(gate_pre, CLAMP_LIMIT)
    up_clip = jnp.clip(up_pre, -CLAMP_LIMIT, CLAMP_LIMIT)
    sigmoid_gate = jax.nn.sigmoid(GATE_SLOPE * gate_clip)
    activated = (gate_clip * sigmoid_gate * (up_clip + 1.0)).astype(jnp.bfloat16)
    down_part = lax.dot_general(activated, routed_grads, (((0,), (0,)), ((), ())), preferred_element_type=jnp.float32)
    act_grad = lax.dot_general(routed_grads, down_w, (((1,), (1,)), ((), ())), preferred_element_type=jnp.float32)
    slope = sigmoid_gate + GATE_SLOPE * gate_clip * sigmoid_gate * (1.0 - sigmoid_gate)
    gate_pre_grad = jnp.where(gate_pre < CLAMP_LIMIT, act_grad * (up_clip + 1.0) * slope, 0.0).astype(jnp.bfloat16)
    up_pre_grad = jnp.where(jnp.abs(up_pre) < CLAMP_LIMIT, act_grad * gate_clip * sigmoid_gate, 0.0).astype(jnp.bfloat16)
    gate_part = lax.dot_general(routed_rows, gate_pre_grad, (((0,), (0,)), ((), ())), preferred_element_type=jnp.float32)
    up_part = lax.dot_general(routed_rows, up_pre_grad, (((0,), (0,)), ((), ())), preferred_element_type=jnp.float32)
    row_count = routed_rows.shape[0]
    group = gate_w.shape[1] // N_TP
    gate_groups = gate_pre_grad.reshape(row_count, N_TP, group).astype(jnp.float32)
    up_groups = up_pre_grad.reshape(row_count, N_TP, group).astype(jnp.float32)
    gate_w_groups = gate_w.reshape(gate_w.shape[0], N_TP, group).astype(jnp.float32)
    up_w_groups = up_w.reshape(up_w.shape[0], N_TP, group).astype(jnp.float32)
    partial_value = jnp.einsum('rtf,dtf->trd', gate_groups, gate_w_groups) + jnp.einsum('rtf,dtf->trd', up_groups, up_w_groups)
    rounded = lax.optimization_barrier(partial_value.astype(jnp.bfloat16))
    back_rows = lax.optimization_barrier(jnp.sum(rounded.astype(jnp.float32), axis=0)).astype(jnp.bfloat16)
    return (gate_part.astype(jnp.bfloat16), up_part.astype(jnp.bfloat16), down_part.astype(jnp.bfloat16), back_rows)

def prepare(query_block, key_block, value_block, decay_block, start):
    cosines, sines = rotation_tables(start, TOK_DEV, KD)
    query_rotated = turn(query_block.astype(jnp.float32), cosines, sines).transpose(1, 0, 2)
    key_rotated = (turn(key_block.astype(jnp.float32), cosines, sines) * KD ** (-0.5)).transpose(1, 0, 2)
    value_per_head = value_block.astype(jnp.float32).transpose(1, 0, 2)
    running_total = jnp.cumsum(decay_block, axis=0).T
    block_total = running_total[:, -1]
    causal = (jnp.arange(TOK_DEV)[:, None] >= jnp.arange(TOK_DEV)[None, :])[None]
    difference = running_total[:, :, None] - running_total[:, None, :]
    decay_mask = jnp.where(causal, jnp.exp(jnp.where(causal, difference, 0.0)), 0.0)
    return (query_rotated, key_rotated, value_per_head, running_total, block_total, decay_mask, cosines, sines)

def reference(stream, out_grad, routes, route_weight, queries, key_vectors, value_vectors, log_decay, out_proj, gate_weight, up_weight, down_weight):
    pair_count = 2 * TOK_DEV
    flat_ids, slot_ids = jax.vmap(lambda block_data: slot_numbers(block_data, EXPERTS))(routes.reshape(N_SP, TOK_DEV, 2))
    destination = flat_ids * CAP + slot_ids

    def place(target):
        return jnp.full((EXPERTS * CAP,), -1, jnp.int32).at[target].set(jnp.arange(pair_count, dtype=jnp.int32))
    source = jax.vmap(place)(destination)
    block_ids = jnp.arange(N_SP, dtype=jnp.int32)[:, None]
    present = source >= 0
    global_pair = jnp.where(present, block_ids * pair_count + source, 0).astype(jnp.int32)
    per_expert = global_pair.reshape(N_SP, EXPERTS, CAP).transpose(1, 0, 2).reshape(EXPERTS, N_SP * CAP)
    occupied = present.reshape(N_SP, EXPERTS, CAP).transpose(1, 0, 2).reshape(EXPERTS, N_SP * CAP)
    pair_grad = (route_weight[:, :, None] * out_grad[:, None, :].astype(jnp.float32)).astype(jnp.bfloat16)
    pair_grad = pair_grad.reshape(2 * SEQUENCE_TOKENS, D)
    zero_value = jnp.zeros((), jnp.bfloat16)

    def one_expert(expert_index):
        pair_ids = per_expert[expert_index]
        row_mask = occupied[expert_index][:, None]
        routed_rows = jnp.where(row_mask, jnp.take(stream, pair_ids // 2, axis=0), zero_value)
        routed_grads = jnp.where(row_mask, jnp.take(pair_grad, pair_ids, axis=0), zero_value)
        return expert_pass(routed_rows, routed_grads, gate_weight[expert_index], up_weight[expert_index], down_weight[expert_index])
    gate_grad, up_grad, down_grad, back_rows = lax.map(one_expert, jnp.arange(EXPERTS, dtype=jnp.int32))
    row_index = (flat_ids * (N_SP * CAP) + block_ids * CAP + slot_ids).astype(jnp.int32)
    per_pair = jnp.take(back_rows.reshape(EXPERTS * N_SP * CAP, D), row_index.reshape(-1), axis=0)
    per_pair = per_pair.reshape(SEQUENCE_TOKENS, 2, D).astype(jnp.float32)
    resid_grad = (out_grad.astype(jnp.float32) + per_pair[:, 0] + per_pair[:, 1]).astype(jnp.bfloat16)

    def to_blocks(array):
        return array.reshape((N_SP, TOK_DEV) + array.shape[1:])
    starts = jnp.arange(N_SP, dtype=jnp.int32) * TOK_DEV
    inputs = (to_blocks(queries), to_blocks(key_vectors), to_blocks(value_vectors), to_blocks(log_decay), starts)

    def forward(running_state, block_data):
        query_rotated, key_rotated, value_per_head, running_total, block_total, decay_mask, cosines, sines = prepare(*block_data)
        weights = jnp.einsum('hik,hjk->hij', query_rotated, key_rotated, precision=TOP_PRECISION) * decay_mask
        retained_output = jnp.einsum('hij,hjv->hiv', weights, value_per_head, precision=TOP_PRECISION)
        retained_output = retained_output + jnp.exp(running_total)[..., None] * jnp.einsum('dzr,drs->dzs', query_rotated, running_state, precision=TOP_PRECISION)
        remaining_decay = jnp.exp(block_total[:, None] - running_total)
        inner_state = jnp.einsum('wfs,wfi->wsi', key_rotated * remaining_decay[..., None], value_per_head, precision=TOP_PRECISION)
        new_state = jnp.exp(block_total)[:, None, None] * running_state + inner_state
        return (new_state, (retained_output, running_state))
    _, (retained_all, incoming_state) = lax.scan(forward, jnp.zeros((RETENTION_HEADS, KD, VD), jnp.float32), inputs)
    inverse_rms = lax.rsqrt(lax.optimization_barrier(jnp.mean(retained_all * retained_all, axis=-1, keepdims=True)) + EPSILON)
    normed = retained_all * inverse_rms
    normed_bf = normed.transpose(0, 2, 1, 3).reshape(SEQUENCE_TOKENS, HV).astype(jnp.bfloat16)
    proj_grad = lax.dot_general(resid_grad, normed_bf, (((0,), (0,)), ((), ())), preferred_element_type=jnp.float32)
    normed_grad = jnp.dot(resid_grad, out_proj, preferred_element_type=jnp.float32)
    normed_grad = normed_grad.reshape(N_SP, TOK_DEV, RETENTION_HEADS, VD).transpose(0, 2, 1, 3)
    retention_gradient = inverse_rms * (normed_grad - normed * lax.optimization_barrier(jnp.mean(normed_grad * normed, axis=-1, keepdims=True)))

    def backward(next_rows, block_data):
        block_inputs, running_state, gradient_tile = block_data
        query_rotated, key_rotated, value_per_head, running_total, block_total, decay_mask, cosines, sines = prepare(*block_inputs)
        per_head_decay = jnp.exp(running_total)
        remaining_decay = jnp.exp(block_total[:, None] - running_total)
        weights = jnp.einsum('hik,hjk->hij', query_rotated, key_rotated, precision=TOP_PRECISION) * decay_mask
        score_grad = jnp.einsum('hiv,hjv->hij', gradient_tile, value_per_head, precision=TOP_PRECISION) * decay_mask
        query_portion = jnp.einsum('hij,hjk->hik', score_grad, key_rotated, precision=TOP_PRECISION)
        query_portion = query_portion + per_head_decay[..., None] * jnp.einsum('bpl,btl->bpt', gradient_tile, running_state, precision=TOP_PRECISION)
        key_portion = jnp.einsum('hij,hik->hjk', score_grad, query_rotated, precision=TOP_PRECISION)
        key_portion = key_portion + remaining_decay[..., None] * jnp.einsum('uxn,ubn->uxb', value_per_head, next_rows, precision=TOP_PRECISION)
        value_portion = jnp.einsum('hij,hiv->hjv', weights, gradient_tile, precision=TOP_PRECISION)
        value_portion = value_portion + remaining_decay[..., None] * jnp.einsum('bui,bim->bum', key_rotated, next_rows, precision=TOP_PRECISION)
        inner_gradient = jnp.einsum('gwn,gwj->gnj', query_rotated * per_head_decay[..., None], gradient_tile, precision=TOP_PRECISION)
        earlier_grad = inner_gradient + jnp.exp(block_total)[:, None, None] * next_rows
        q_out = turn(query_portion.transpose(1, 0, 2), cosines, -sines).astype(jnp.bfloat16)
        k_out = (turn(key_portion.transpose(1, 0, 2), cosines, -sines) * KD ** (-0.5)).astype(jnp.bfloat16)
        v_out = value_portion.transpose(1, 0, 2).astype(jnp.bfloat16)
        return (earlier_grad, (q_out, k_out, v_out))
    _, (query_grad, key_grad, value_grad) = lax.scan(backward, jnp.zeros((RETENTION_HEADS, KD, VD), jnp.float32), (inputs, incoming_state, retention_gradient), reverse=True)
    query_grad = query_grad.reshape(SEQUENCE_TOKENS, RETENTION_HEADS, KD)
    key_grad = key_grad.reshape(SEQUENCE_TOKENS, RETENTION_HEADS, KD)
    value_grad = value_grad.reshape(SEQUENCE_TOKENS, RETENTION_HEADS, VD)
    return (gate_grad, up_grad, down_grad, proj_grad, query_grad, key_grad, value_grad)
```

```python
import functools

import jax
import jax.numpy as jnp
from jax import lax
from jax.experimental import pallas as pl
from jax.experimental.pallas import tpu as pltpu
from jax.sharding import PartitionSpec as P

CLAMP_LIMIT = 7.0
GATE_SLOPE = 1.702
EPSILON = 1e-06
F32 = jnp.float32
BF16 = jnp.bfloat16
MESH = pl.DeviceIdType.MESH


def any_specs(count):
    return [pl.BlockSpec(memory_space=pl.ANY)] * count


def vmem_specs(count):
    return [pl.BlockSpec(memory_space=pltpu.VMEM)] * count


def tp_partners(c, n_tp):
    far = lax.rem(c + n_tp // 2, n_tp)
    near = c + 1 - 2 * lax.rem(c, 2)
    return far, near


def greet(n_sp, me, c, sp_peers, tp_peers):
    barrier = pltpu.get_barrier_semaphore()
    count = 0
    if sp_peers:
        for k in range(1, n_sp):
            pl.semaphore_signal(
                barrier, inc=1, device_id=(lax.rem(me + k, n_sp), c), device_id_type=MESH
            )
            count += 1
    for t in tp_peers:
        pl.semaphore_signal(barrier, inc=1, device_id=(me, t), device_id_type=MESH)
        count += 1
    pl.semaphore_wait(barrier, count)


def push(src, dst, send_sem, recv_sem, device):
    return pltpu.make_async_remote_copy(
        src_ref=src,
        dst_ref=dst,
        send_sem=send_sem,
        recv_sem=recv_sem,
        device_id=device,
        device_id_type=MESH,
    )


class Chain:
    def __init__(self, src, out, n_sp, me, c, sems, ways):
        self.src, self.out, self.me, self.c = src, out, me, c
        self.pairs, self.ways = n_sp // 2, ways
        self.pair = me // 2
        self.other = me + 1 - 2 * lax.rem(me, 2)
        self.zs, self.zr, self.ys, self.yr, self.own_sem = sems

    def has(self, d, way):
        return self.pair >= d if way == 0 else self.pair + d < self.pairs

    def room(self, way):
        return self.pair + 1 < self.pairs if way == 0 else self.pair >= 1

    def spot(self, base, d, way):
        return self.out.at[base - 2 * d if way == 0 else base + 2 * d]

    def along(self, d, way):
        spot = self.spot(self.me, d, way)
        return push(
            self.src if d == 0 else spot, spot, self.zs.at[way, d], self.zr.at[way, d + 1],
            (self.me + 2 if way == 0 else self.me - 2, self.c),
        )

    def across(self, d, way):
        spot = self.spot(self.me, d, way)
        return push(
            self.src if d == 0 else spot, spot, self.ys.at[way, d], self.yr.at[way, d],
            (self.other, self.c),
        )

    def own(self):
        return pltpu.make_async_copy(self.src, self.out.at[self.me], self.own_sem.at[0])

    def each(self, d, act):
        for way in self.ways:

            @pl.when(self.has(d, way))
            def _():
                if d < self.pairs - 1:

                    @pl.when(self.room(way))
                    def _():
                        act(self.along(d, way))

                if d > 0 or way == self.ways[0]:
                    act(self.across(d, way))

    def start(self):
        self.own().start()
        self.each(0, lambda cp: cp.start())

    def step(self, d):
        for way in self.ways:

            @pl.when(self.has(d, way))
            def _():
                spot = self.spot(self.me, d, way)
                push(
                    spot, spot, self.zs.at[way, d], self.zr.at[way, d], (self.other, self.c)
                ).wait_recv()

        self.each(d, lambda cp: cp.start())

    def finish(self):
        for d in range(self.pairs):
            for way in self.ways:
                if d == 0 and way != self.ways[0]:
                    continue

                @pl.when(self.has(d, way))
                def _():
                    spot = self.spot(self.other, d, way)
                    push(
                        spot, spot, self.ys.at[way, d], self.yr.at[way, d], (self.other, self.c)
                    ).wait_recv()

            self.each(d, lambda cp: cp.wait_send())
        self.own().wait()


def chain_sems(n_sp):
    dma = pltpu.SemaphoreType.DMA
    return [dma((2, n_sp // 2))] * 4 + [dma((1,))]


def dot(a, b, da, db):
    return lax.dot_general(a, b, (((da,), (db,)), ((), ())), preferred_element_type=F32)


def flat(block):
    n, cap, q = block.shape
    if cap % 16 == 0:
        return block.reshape(n * cap, q)
    return block.astype(F32).reshape(n * cap, q).astype(BF16)


def experts_kernel(
    n_sp, n_tp, pack, pick, og, gate_w, up_w, down_w, tot, state,
    gate_o, up_o, down_o, resid, tot_out, states,
    full, gu, dw, act, gug, back, part, xbuf, xrecv, sendbuf, ret, resq, gout, uout, dout,
    wsem, osem, own_sem, ssem, rsem, fs, fr, ns, nr, es, er, ps, pr, xs, xr, hs, hr,
    gs, gr, tssem, trsem, *chain_sem,
):
    me = lax.axis_index("sp")
    c = lax.axis_index("tp")
    far, near = tp_partners(c, n_tp)
    near_far = lax.rem(near + n_tp // 2, n_tp)
    cap, q = pack.shape[2:]
    hid = dw.shape[0]
    loads = [
        pltpu.make_async_copy(gate_w.at[0], gu.at[:, pl.ds(0, hid)], wsem.at[0]),
        pltpu.make_async_copy(up_w.at[0], gu.at[:, pl.ds(hid, hid)], wsem.at[1]),
        pltpu.make_async_copy(down_w.at[0], dw, wsem.at[2]),
    ]
    for cp in loads:
        cp.start()
    greet(n_sp, me, c, True, (far, near))

    def source(k):
        return lax.rem(me + n_sp - k, n_sp)

    def out_copy(k):
        peer = lax.rem(me + k, n_sp)
        return push(pack.at[peer], full.at[me, c], ssem.at[k], rsem.at[k], (peer, c))

    def tot_copy(k):
        peer = lax.rem(me + k, n_sp)
        return push(tot, tot_out.at[me], tssem.at[k], trsem.at[k], (peer, c))

    def far_copy(k, quarter, own=False):
        spot = full.at[source(k), quarter]
        return push(pack.at[me] if own else spot, spot, fs.at[k], fr.at[k], (me, far))

    def near_copy(k, quarter, own=False):
        spot = full.at[source(k), quarter]
        return push(pack.at[me] if own else spot, spot, ns.at[k], nr.at[k], (me, near))

    def relay_copy(k, quarter):
        spot = full.at[source(k), quarter]
        return push(spot, spot, es.at[k], er.at[k], (me, near))

    def part_copy(k, b):
        quarter = near_far if b == 0 else near
        return push(
            back.at[k, quarter], part.at[b, k], ps.at[b, k], pr.at[b, k], (me, near)
        )

    def x_copy(k):
        return push(xbuf.at[k], xrecv.at[k], xs.at[k], xr.at[k], (me, far))

    def home_copy(k):
        return push(sendbuf.at[k], ret.at[me], hs.at[k], hr.at[k], (source(k), c))

    far_copy(0, c, True).start()
    near_copy(0, c, True).start()
    for k in range(1, n_sp):
        out_copy(k).start()
    for k in range(1, n_sp):
        tot_copy(k).start()
    own_tot = pltpu.make_async_copy(tot, tot_out.at[me], own_sem.at[0])
    own_tot.start()
    chain = Chain(state, states, n_sp, me, c, chain_sem, (0,))
    chain.start()
    full[me, c] = pack[me]
    for cp in loads:
        cp.wait()

    def compute(k):
        src = source(k)
        near_copy(k, near).wait_recv()
        relay_copy(k, near_far).wait_recv()
        pre = None
        act_grad = None
        for t in range(n_tp):
            cols = pl.ds(t * q, q)
            a = dot(full[src, t, 0], gu[cols, :], 1, 0)
            b = dot(full[src, t, 1], dw[:, cols], 1, 1)
            pre = a if t == 0 else pre + a
            act_grad = b if t == 0 else act_grad + b
        gate_pre = pre[:, :hid]
        up_pre = pre[:, hid:]
        gate_clip = jnp.minimum(gate_pre, CLAMP_LIMIT)
        up_clip = jnp.clip(up_pre, -CLAMP_LIMIT, CLAMP_LIMIT)
        sig = 1.0 / (1.0 + jnp.exp(-GATE_SLOPE * gate_clip))
        gated = gate_clip * sig
        act[src] = (gated * (up_clip + 1.0)).astype(BF16)
        slope = sig + GATE_SLOPE * gated * (1.0 - sig)
        gpg = jnp.where(gate_pre < CLAMP_LIMIT, act_grad * (up_clip + 1.0) * slope, 0.0)
        upg = jnp.where(jnp.abs(up_pre) < CLAMP_LIMIT, act_grad * gated, 0.0)
        both = jnp.concatenate([gpg, upg], axis=1).astype(BF16)
        gug[src] = both
        for t in range(n_tp):
            back[k, t] = dot(both, gu[pl.ds(t * q, q), :], 1, 1).astype(BF16)

    def first(k):
        part_copy(k, 0).wait_recv()
        xbuf[k] = (back[k, far].astype(F32) + part[0, k].astype(F32)).astype(BF16)
        x_copy(k).start()

    def second(k):
        part_copy(k, 1).wait_recv()
        x_copy(k).wait_recv()
        total = (
            back[k, c].astype(F32) + part[1, k].astype(F32) + xrecv[k].astype(F32)
        ).astype(BF16)

        @pl.when(k == 0)
        def _():
            ret[me] = total

        @pl.when(k > 0)
        def _():
            sendbuf[k] = total
            home_copy(k).start()

    def relay_far(k):
        far_copy(k, far).wait_recv()
        relay_copy(k, far).start()

    def step(n, carry):
        @pl.when((n >= 1) & (n < n_sp))
        def _():
            out_copy(n).wait_recv()
            far_copy(n, c).start()
            near_copy(n, c).start()

        @pl.when((n >= 1) & (n <= n_sp))
        def _():
            relay_far(n - 1)

        for d in range(1, n_sp // 2):

            @pl.when(n == 2 * d)
            def _():
                chain.step(d)

        @pl.when((n >= 2) & (n < n_sp + 2))
        def _():
            compute(n - 2)
            part_copy(n - 2, 0).start()
            part_copy(n - 2, 1).start()

        @pl.when((n >= 3) & (n < n_sp + 3))
        def _():
            first(n - 3)

        @pl.when((n >= 4) & (n < n_sp + 4))
        def _():
            second(n - 4)

        return carry

    lax.fori_loop(0, n_sp + 4, step, 0)

    def weights_grad(t, carry):
        cols = pl.ds(pl.multiple_of(t * q, 128), q)
        x = flat(full[:, t, 0])
        g = flat(full[:, t, 1])
        both = dot(x, flat(gug[...]), 0, 0).astype(BF16)
        gout[cols, :] = both[:, :hid]
        uout[cols, :] = both[:, hid:]
        dout[:, cols] = dot(flat(act[...]), g, 0, 0).astype(BF16)
        return carry

    lax.fori_loop(0, n_tp, weights_grad, 0)
    stores = [
        pltpu.make_async_copy(gout, gate_o.at[0], osem.at[0]),
        pltpu.make_async_copy(uout, up_o.at[0], osem.at[1]),
        pltpu.make_async_copy(dout, down_o.at[0], osem.at[2]),
    ]
    for cp in stores:
        cp.start()

    def arrive(k, carry):
        home = lax.rem(me + k, n_sp)
        push(sendbuf.at[k], ret.at[home], hs.at[k], hr.at[k], (home, c)).wait_recv()
        return carry

    lax.fori_loop(1, n_sp, arrive, 0)
    resq[...] = (og[...].astype(F32) + dot(pick[...], flat(ret[...]), 0, 0)).astype(BF16)

    def cols(quarter):
        return pl.ds(pl.multiple_of(quarter * q, 128), q)

    mine = resid.at[:, cols(c)]
    to_far = push(resq, mine, gs.at[0], gr.at[0], (me, far))
    to_near = push(resq, mine, gs.at[1], gr.at[1], (me, near))
    to_far.start()
    to_near.start()
    resid[:, cols(c)] = resq[...]
    spot = resid.at[:, cols(far)]
    push(resq, spot, gs.at[0], gr.at[0], (me, far)).wait_recv()
    onward = push(spot, spot, gs.at[2], gr.at[2], (me, near))
    onward.start()
    push(resq, resid.at[:, cols(near)], gs.at[1], gr.at[1], (me, near)).wait_recv()
    push(resq, resid.at[:, cols(near_far)], gs.at[2], gr.at[2], (me, near)).wait_recv()

    for cp in (to_far, to_near, onward):
        cp.wait_send()

    def drain(k, carry):
        far_copy(k, c).wait_send()
        near_copy(k, c).wait_send()
        relay_copy(k, far).wait_send()
        part_copy(k, 0).wait_send()
        part_copy(k, 1).wait_send()
        x_copy(k).wait_send()

        @pl.when(k > 0)
        def _():
            out_copy(k).wait_send()
            home_copy(k).wait_send()
            tot_copy(k).wait_send()
            peer = source(k)
            push(tot, tot_out.at[peer], tssem.at[k], trsem.at[k], (peer, c)).wait_recv()

        return carry

    lax.fori_loop(0, n_sp, drain, 0)
    own_tot.wait()
    chain.finish()
    for cp in stores:
        cp.wait()


def experts(pack, pick, og_q, gate_weight, up_weight, down_weight, tot, state, n_tp):
    n_sp, _, cap, q = pack.shape
    tokens = og_q.shape[0]
    width = q * n_tp
    hid = gate_weight.shape[2]
    dma = pltpu.SemaphoreType.DMA
    block = pltpu.VMEM((n_sp, cap, q), BF16)
    vmem = pltpu.VMEM
    return pl.pallas_call(
        functools.partial(experts_kernel, n_sp, n_tp),
        out_shape=(
            jax.ShapeDtypeStruct(gate_weight.shape, BF16),
            jax.ShapeDtypeStruct(up_weight.shape, BF16),
            jax.ShapeDtypeStruct(down_weight.shape, BF16),
            jax.ShapeDtypeStruct((tokens, width), BF16),
            jax.ShapeDtypeStruct((n_sp,) + tot.shape, tot.dtype),
            jax.ShapeDtypeStruct((n_sp,) + state.shape, state.dtype),
        ),
        in_specs=vmem_specs(3) + any_specs(5),
        out_specs=tuple(any_specs(3) + vmem_specs(1) + any_specs(2)),
        scratch_shapes=[
            vmem((n_sp, n_tp, 2, cap, q), BF16),
            vmem((width, 2 * hid), BF16),
            vmem((hid, width), BF16),
            vmem((n_sp, cap, hid), BF16),
            vmem((n_sp, cap, 2 * hid), BF16),
            vmem((n_sp, n_tp, cap, q), BF16),
            vmem((2, n_sp, cap, q), BF16),
            block, block, block, block,
            vmem((tokens, q), BF16),
            vmem((width, hid), BF16),
            vmem((width, hid), BF16),
            vmem((hid, width), BF16),
            dma((3,)), dma((3,)), dma((1,)),
        ]
        + [dma((n_sp,))] * 8
        + [dma((2, n_sp))] * 2
        + [dma((n_sp,))] * 4
        + [dma((3,))] * 2
        + [dma((n_sp,))] * 2
        + chain_sems(n_sp),
        compiler_params=pltpu.CompilerParams(
            collective_id=0, has_side_effects=True, vmem_limit_bytes=56 * 2**20
        ),
        name="experts",
    )(pack, pick, og_q, gate_weight, up_weight, down_weight, tot, state)


def swap_kernel(
    n_sp, w, resid, state, normed, cols_out, states, normed_all, own_sem, ssem, rsem, *chain_sem
):
    me = lax.axis_index("sp")
    c = lax.axis_index("tp")
    greet(n_sp, me, c, True, ())

    def part(index):
        if len(resid.shape) == 3:
            return resid.at[index]
        return resid.at[:, pl.ds(pl.multiple_of(index * w, 128), w)]

    chain = Chain(state, states, n_sp, me, c, chain_sem[:5], (1,))
    chain.start()
    spread = Chain(normed, normed_all, n_sp, me, c, chain_sem[5:], (0, 1))
    spread.start()
    waits = []

    def send(k):
        peer = lax.rem(me + k, n_sp)
        cp = push(part(peer), cols_out.at[me], ssem.at[k], rsem.at[k], (peer, c))
        cp.start()
        waits.append(cp)

    local = pltpu.make_async_copy(part(me), cols_out.at[me], own_sem.at[0])
    local.start()
    for d in range(1, n_sp // 2):
        send(2 * d)
        send(2 * d - 1)
        chain.step(d)
        spread.step(d)
    send(n_sp - 1)
    for k in range(1, n_sp):
        source = lax.rem(me + n_sp - k, n_sp)
        spot = cols_out.at[source]
        push(spot, spot, ssem.at[k], rsem.at[k], (source, c)).wait_recv()
    for cp in waits:
        cp.wait_send()
    local.wait()
    chain.finish()
    spread.finish()


def swap(resid, state, normed, n_sp):
    tokens, width = resid.shape
    w = width // n_sp
    if w % 128:
        resid = resid.reshape(tokens, n_sp, w).transpose(1, 0, 2)
    dma = pltpu.SemaphoreType.DMA
    return pl.pallas_call(
        functools.partial(swap_kernel, n_sp, w),
        out_shape=(
            jax.ShapeDtypeStruct((n_sp, tokens, w), BF16),
            jax.ShapeDtypeStruct((n_sp,) + state.shape, BF16),
            jax.ShapeDtypeStruct((n_sp,) + normed.shape, BF16),
        ),
        in_specs=any_specs(3),
        out_specs=tuple(any_specs(3)),
        scratch_shapes=[dma((1,)), dma((n_sp,)), dma((n_sp,))] + chain_sems(n_sp) * 2,
        compiler_params=pltpu.CompilerParams(collective_id=2, has_side_effects=True),
        name="swap",
    )(resid, state, normed)


def rotation_tables(start, count, key_width):
    frequency = 1.0 / 10000.0 ** jnp.linspace(0.0, 1.0, key_width // 2, dtype=F32)
    frequency = jnp.repeat(frequency, 2)
    token_position = (start + jnp.arange(count, dtype=jnp.int32)).astype(F32)
    angles = token_position[:, None] * frequency[None, :]
    return (jnp.cos(angles)[None], jnp.sin(angles)[None])


def swap_matrix(key_width):
    row = jnp.arange(key_width)[:, None]
    col = jnp.arange(key_width)[None, :]
    up = (col == row + 1) & (row % 2 == 0)
    down = (col == row - 1) & (row % 2 == 1)
    return (up.astype(F32) - down.astype(F32)).astype(BF16)


def turn(field, cosines, sines, matrix):
    turned = jnp.einsum("htk,kl->htl", field.astype(BF16), matrix, preferred_element_type=F32)
    return field.astype(F32) * cosines + turned * sines


def ein(spec, a, b):
    return jnp.einsum(spec, a.astype(BF16), b.astype(BF16), preferred_element_type=F32)


def fine(spec, a, b):
    return jnp.einsum(spec, a.astype(F32), b.astype(F32), precision=lax.Precision.HIGHEST)


def weighted(states, factors, present):
    kept = jnp.where(present[:, None, None, None], states.astype(F32), 0.0)
    return jnp.sum(kept * factors[:, :, None, None], axis=0)


def mm(a, b, da, db):
    return lax.dot_general(a, b, (((da,), (db,)), ((), ())), preferred_element_type=F32)


def per_device(
    stream, out_grad, routes, route_weight, queries, key_vectors, value_vectors, log_decay,
    out_proj, gate_weight, up_weight, down_weight,
):
    n_sp = lax.axis_size("sp")
    n_tp = lax.axis_size("tp")
    me = lax.axis_index("sp")
    tokens, width = stream.shape
    capacity = 4 * tokens // n_sp
    slots = n_sp * capacity
    quarter = width // n_tp
    heads = queries.shape[1]
    key_width = queries.shape[2]
    value_width = value_vectors.shape[2]

    ids = jnp.arange(n_sp, dtype=jnp.int32)
    chosen = routes[:, :, None] == ids[None, None, :]
    counts = jnp.sum(chosen.astype(F32), axis=1).astype(BF16)
    place = jnp.arange(tokens)
    lower = (place[:, None] > place[None, :]).astype(BF16)
    before = jnp.dot(lower, counts, preferred_element_type=F32)
    slot = jnp.sum(jnp.where(chosen, before[:, None, :], 0.0), axis=2).astype(jnp.int32)
    target = routes * capacity + slot
    spots = jnp.arange(slots, dtype=jnp.int32)
    hit = target.T[:, None, :] == spots[None, :, None]
    pick = (hit[0] | hit[1]).astype(BF16)
    weight = jnp.sum(
        jnp.where(hit[0], route_weight[None, :, 0], 0.0)
        + jnp.where(hit[1], route_weight[None, :, 1], 0.0),
        axis=1,
    )
    col_start = lax.axis_index("tp") * quarter
    stream_q = lax.dynamic_slice_in_dim(stream, col_start, quarter, 1)
    og_q = lax.dynamic_slice_in_dim(out_grad, col_start, quarter, 1)
    send_rows = jnp.dot(pick, stream_q, preferred_element_type=F32).astype(BF16)
    send_grads = (
        weight[:, None] * jnp.dot(pick, og_q, preferred_element_type=F32)
    ).astype(BF16)

    running = jnp.cumsum(log_decay, axis=0).T
    block_total = running[:, -1]
    tot = jnp.broadcast_to(jnp.pad(block_total, (0, 128 - heads))[None, :], (8, 128))
    matrix = swap_matrix(key_width)
    cosines, sines = rotation_tables(me * tokens, tokens, key_width)
    scale = key_width ** (-0.5)
    query_rot = turn(queries.transpose(1, 0, 2), cosines, sines, matrix)
    key_rot = turn(key_vectors.transpose(1, 0, 2), cosines, sines, matrix) * scale
    values = value_vectors.transpose(1, 0, 2)
    causal = (place[:, None] >= place[None, :])[None]
    difference = running[:, :, None] - running[:, None, :]
    mask = jnp.where(causal, jnp.exp(jnp.where(causal, difference, 0.0)), 0.0)
    decay = jnp.exp(running)[..., None]
    remaining = jnp.exp(block_total[:, None] - running)[..., None]
    inner = ein("wfs,wfi->wsi", key_rot * remaining, values).astype(BF16)
    pack = jnp.stack(
        [send_rows.reshape(n_sp, capacity, quarter), send_grads.reshape(n_sp, capacity, quarter)],
        axis=1,
    )
    gate_part, up_part, down_part, resid, tots, inner_all = experts(
        pack, pick, og_q, gate_weight, up_weight, down_weight, tot, inner, n_tp
    )
    key_bf = key_rot.astype(BF16)
    query_bf = query_rot.astype(BF16)
    weights = fine("hik,hjk->hij", query_rot, key_rot) * mask
    retained_local = fine("hij,hjv->hiv", weights, values)

    totals = tots[:, 0, :heads]
    sums = jnp.cumsum(totals, axis=0)
    sum_before = jnp.sum(jnp.where((ids < me)[:, None], totals, 0.0), axis=0)
    sum_through = sum_before + block_total
    past = jnp.where((ids < me)[:, None], sum_before[None] - sums, 0.0)
    past = jnp.where((ids < me)[:, None], jnp.exp(past), 0.0)
    coming = jnp.where((ids > me)[:, None], sums - totals - sum_through[None], 0.0)
    coming = jnp.where((ids > me)[:, None], jnp.exp(coming), 0.0)
    incoming = weighted(inner_all, past, ids < me)
    retained = retained_local + decay * fine("dzr,drs->dzs", query_rot, incoming)
    inverse_rms = lax.rsqrt(jnp.mean(retained * retained, axis=-1, keepdims=True) + EPSILON)
    normed = retained * inverse_rms
    normed_bf = normed.transpose(1, 0, 2).reshape(tokens, heads * value_width).astype(BF16)

    normed_grad = jnp.dot(resid, out_proj, preferred_element_type=F32)
    normed_grad = normed_grad.reshape(tokens, heads, value_width).transpose(1, 0, 2)
    grad = inverse_rms * (
        normed_grad - normed * jnp.mean(normed_grad * normed, axis=-1, keepdims=True)
    )
    grad_bf = grad.astype(BF16)
    inner_grad = ein("gwn,gwj->gnj", query_rot * decay, grad_bf).astype(BF16)
    resid_cols, grads_all, normed_all = swap(resid, inner_grad, normed_bf, n_sp)
    future = weighted(grads_all, coming, ids > me).astype(BF16)
    score = fine("hiv,hjv->hij", grad, values) * mask
    query_portion = ein("hij,hjk->hik", score, key_bf) + decay * fine(
        "bpl,btl->bpt", grad, incoming
    )
    key_portion = ein("hij,hik->hjk", score, query_bf) + remaining * ein(
        "uxn,ubn->uxb", values, future
    )
    value_portion = ein("hij,hiv->hjv", weights, grad_bf) + remaining * ein(
        "bui,bim->bum", key_bf, future
    )
    query_grad = turn(query_portion, cosines, -sines, matrix).astype(BF16).transpose(1, 0, 2)
    key_grad = (
        (turn(key_portion, cosines, -sines, matrix) * scale).astype(BF16).transpose(1, 0, 2)
    )
    value_grad = value_portion.astype(BF16).transpose(1, 0, 2)
    proj_grad = mm(
        resid_cols.reshape(n_sp * tokens, -1), normed_all.reshape(n_sp * tokens, -1), 0, 0
    )
    return (
        gate_part,
        up_part,
        down_part,
        proj_grad,
        query_grad,
        key_grad,
        value_grad,
    )


def solution(mesh):
    in_specs = (
        P("sp", None),
        P("sp", None),
        P("sp", None),
        P("sp", None),
        P("sp", "tp", None),
        P("sp", "tp", None),
        P("sp", "tp", None),
        P("sp", "tp"),
        P(None, "tp"),
        P("sp", None, "tp"),
        P("sp", None, "tp"),
        P("sp", "tp", None),
    )
    out_specs = (
        P("sp", None, "tp"),
        P("sp", None, "tp"),
        P("sp", "tp", None),
        P("sp", "tp"),
        P("sp", "tp", None),
        P("sp", "tp", None),
        P("sp", "tp", None),
    )
    return jax.shard_map(
        per_device, mesh=mesh, in_specs=in_specs, out_specs=out_specs, check_vma=False
    )
```

```python
import functools

import jax
import jax.numpy as jnp
import numpy as np
from jax import lax
from jax.experimental import pallas as pl
from jax.experimental.pallas import tpu as pltpu
from jax.sharding import PartitionSpec as P

CLAMP_LIMIT = 7.0
GATE_SLOPE = 1.702
EPSILON = 1e-06
F32 = jnp.float32
BF16 = jnp.bfloat16
MESH = pl.DeviceIdType.MESH
SPLIT = 2


def any_specs(count):
    return [pl.BlockSpec(memory_space=pl.ANY)] * count


def vmem_specs(count):
    return [pl.BlockSpec(memory_space=pltpu.VMEM)] * count


def push(src, dst, send_sem, recv_sem, device):
    return pltpu.make_async_remote_copy(
        src_ref=src,
        dst_ref=dst,
        send_sem=send_sem,
        recv_sem=recv_sem,
        device_id=device,
        device_id_type=MESH,
    )


class Chain:
    def __init__(self, src, out, n_sp, me, c, sems, ways):
        self.src, self.out, self.me, self.c = src, out, me, c
        self.pairs, self.ways = n_sp // 2, ways
        self.pair = me // 2
        self.other = me + 1 - 2 * lax.rem(me, 2)
        self.zs, self.zr, self.ys, self.yr = sems

    def has(self, d, way):
        return self.pair >= d if way == 0 else self.pair + d < self.pairs

    def room(self, way):
        return self.pair + 1 < self.pairs if way == 0 else self.pair >= 1

    def spot(self, base, d, way):
        return self.out.at[base - 2 * d if way == 0 else base + 2 * d]

    def along(self, d, way):
        spot = self.spot(self.me, d, way)
        return push(
            self.src if d == 0 else spot, spot, self.zs.at[way, d], self.zr.at[way, d + 1],
            (self.me + 2 if way == 0 else self.me - 2, self.c),
        )

    def across(self, d, way):
        spot = self.spot(self.me, d, way)
        return push(
            self.src if d == 0 else spot, spot, self.ys.at[way, d], self.yr.at[way, d],
            (self.other, self.c),
        )

    def each(self, d, act):
        for way in self.ways:

            @pl.when(self.has(d, way))
            def _():
                if d < self.pairs - 1:

                    @pl.when(self.room(way))
                    def _():
                        act(self.along(d, way))

                if d > 0 or way == self.ways[0]:
                    act(self.across(d, way))

    def start(self):
        self.each(0, lambda cp: cp.start())

    def step(self, d):
        for way in self.ways:

            @pl.when(self.has(d, way))
            def _():
                spot = self.spot(self.me, d, way)
                push(
                    spot, spot, self.zs.at[way, d], self.zr.at[way, d], (self.other, self.c)
                ).wait_recv()

        self.each(d, lambda cp: cp.start())

    def finish(self):
        for d in range(self.pairs):
            for way in self.ways:
                if d == 0 and way != self.ways[0]:
                    continue

                @pl.when(self.has(d, way))
                def _():
                    spot = self.spot(self.other, d, way)
                    push(
                        spot, spot, self.ys.at[way, d], self.yr.at[way, d], (self.other, self.c)
                    ).wait_recv()

            self.each(d, lambda cp: cp.wait_send())


class Scan:
    def __init__(self, forward, n_sp, me, c, bufs, sems, totals, heads):
        self.forward, self.me, self.c = forward, me, c
        self.zin, self.zout, self.min, self.mout = bufs
        self.zs, self.zr, self.ms, self.mr = sems
        self.own_tot, self.other_tot = totals
        pairs = n_sp // 2
        pair = me // 2
        parity = lax.rem(me, 2)
        self.other = me + 1 - 2 * parity
        self.prev = pair > 0 if forward else pair + 1 < pairs
        self.next = pair + 1 < pairs if forward else pair > 0
        self.ahead = me + 2 if forward else me - 2
        self.slot = pair if forward else pairs - 1 - pair
        self.inside = jnp.where(parity == (0 if forward else 1), 1.0, 0.0)
        self.count = heads * SPLIT

    def z_copy(self, j):
        return push(
            self.zout.at[j], self.zin.at[j], self.zs.at[j], self.zr.at[j], (self.ahead, self.c)
        )

    def m_copy(self, j):
        return push(
            self.mout.at[j], self.min.at[j], self.ms.at[j], self.mr.at[j], (self.other, self.c)
        )

    def clear(self):
        @pl.when(jnp.logical_not(self.prev))
        def _():
            self.zin[...] = jnp.zeros_like(self.zin)

    def decays(self, j):
        h = j // SPLIT
        return jnp.exp(self.own_tot[h, 0:1, 0:1]), jnp.exp(self.other_tot[h, 0:1, 0:1])

    def step(self, own):
        s = self.inside
        for j in range(self.count):
            mine, others = self.decays(j)

            @pl.when(self.prev)
            def _():
                self.z_copy(j).wait_recv()

            z = self.zin[j].astype(F32)
            i = own[j]
            self.zout[j] = (mine * others * z + (s * others + (1.0 - s)) * i).astype(BF16)

            @pl.when(self.next)
            def _():
                self.z_copy(j).start()

            self.mout[j] = ((s * mine + (1.0 - s)) * z + s * i).astype(BF16)
            self.m_copy(j).start()

    def result(self, j):
        s = self.inside
        others = self.decays(j)[1]
        self.m_copy(j).wait_recv()
        z = self.zin[j].astype(F32)
        return (self.min[j].astype(F32) + (s + (1.0 - s) * others) * z).astype(BF16)

    def finish(self):
        for j in range(self.count):

            @pl.when(self.next)
            def _():
                self.z_copy(j).wait_send()

            self.m_copy(j).wait_send()


def dot(a, b, da, db):
    return lax.dot_general(a, b, (((da,), (db,)), ((), ())), preferred_element_type=F32)


def flat(block):
    n, cap, q = block.shape
    if cap % 16 == 0:
        return block.reshape(n * cap, q)
    return block.astype(F32).reshape(n * cap, q).astype(BF16)


def swapped(x):
    width = x.shape[1]
    even = lax.rem(lax.broadcasted_iota(jnp.int32, x.shape, 1), 2) == 0
    return jnp.where(even, -pltpu.roll(x, width - 1, 1), pltpu.roll(x, 1, 1))


def whole_kernel(
    n_sp, n_tp, heads,
    stream, og, routes, route_w, queries, keys, values, log_decay, cos_t, sin_t, cos_s, sin_s,
    gate_w, up_w, down_w, proj_w,
    gate_o, up_o, down_o, proj_o, query_o, key_o, value_o,
    full, pack, gu, dw, pw, act, gug, back, part, xbuf, xrecv, sendbuf, ret, gout, uout, dout,
    pick, wcol, slotmap, weight_map, resid, rcols, normed_own, normed_all, normed_f, inv, dec, rem_,
    mask, wts, qr, kr, cosb, sinb, totb, toto, inner, inner_g, incoming, proj,
    fzin, fzout, fmin, fmout, bzin, bzout, bmin, bmout,
    wsem, osem, tsem, ssem, rsem, fs, fr, ns, nr, es, er, ps, pr, xs, xr, hs, hr, gs, gr,
    cs, cr, ds, dr, *more,
):
    fsem, bsem, chain_sem = more[0:4], more[4:8], more[8:12]
    me = lax.axis_index("sp")
    c = lax.axis_index("tp")
    core, plane = lax.rem(c, 2), c // 2
    ocore, oplane = 1 - core, 1 - plane
    far = lax.rem(c + n_tp // 2, n_tp)
    near = c + 1 - 2 * core
    other = me + 1 - 2 * lax.rem(me, 2)
    cap, q = full.shape[4:]
    hid = dw.shape[0]
    tokens = stream.shape[0]
    kd = cos_t.shape[1]
    vd = values.shape[1] // heads
    scale = kd ** (-0.5)
    bits = [1 << b for b in range((n_sp - 1).bit_length())]

    def peer(k):
        out = 0
        for b in bits:
            out = out + b * lax.rem(me // b + k // b, 2)
        return out

    loads = [
        pltpu.make_async_copy(gate_w.at[0], gu.at[:, pl.ds(0, hid)], wsem.at[0]),
        pltpu.make_async_copy(up_w.at[0], gu.at[:, pl.ds(hid, hid)], wsem.at[1]),
        pltpu.make_async_copy(down_w.at[0], dw, wsem.at[2]),
        pltpu.make_async_copy(proj_w, pw, wsem.at[3]),
    ]
    for cp in loads:
        cp.start()
    barrier = pltpu.get_barrier_semaphore()

    def hello(k, carry):
        pl.semaphore_signal(barrier, inc=1, device_id=(peer(k), c), device_id_type=MESH)
        return carry

    lax.fori_loop(1, n_sp, hello, 0)
    for t in (far, near):
        pl.semaphore_signal(barrier, inc=1, device_id=(me, t), device_id_type=MESH)

    def cols(index):
        return pl.ds(pl.multiple_of(index * q, 128), q)

    expert = lax.broadcasted_iota(jnp.int32, (n_sp, tokens), 0)
    first_of = expert == routes[0:1, :]
    second_of = expert == routes[1:2, :]
    chosen = first_of | second_of
    weight_map[...] = jnp.where(first_of, route_w[0:1, :], 0.0) + jnp.where(
        second_of, route_w[1:2, :], 0.0
    )
    row = lax.broadcasted_iota(jnp.int32, (tokens, tokens), 0)
    col = lax.broadcasted_iota(jnp.int32, (tokens, tokens), 1)
    earlier = jnp.where(row < col, 1.0, 0.0).astype(BF16)
    before = dot(jnp.where(chosen, 1.0, 0.0).astype(BF16), earlier, 1, 0)
    slotmap[...] = jnp.where(chosen, before, -1.0)
    place = lax.broadcasted_iota(jnp.int32, (cap, tokens), 0).astype(F32)
    for e in range(n_sp):
        hit = jnp.where(slotmap[e : e + 1, :] == place, 1.0, 0.0)
        pick[e] = hit.astype(BF16)
        wcol[e] = jnp.sum(hit * weight_map[e : e + 1, :], axis=1, keepdims=True)

    def fill(spot, e, index):
        rows = dot(pick[e], stream[:, cols(index)], 1, 0)
        grads = wcol[e] * dot(pick[e], og[:, cols(index)], 1, 0)
        spot[0] = rows.astype(BF16)
        spot[1] = grads.astype(BF16)

    def out_copy(k):
        return push(
            pack.at[k, plane], full.at[me, core, plane], ssem.at[k], rsem.at[k], (peer(k), c)
        )

    def out_pair():
        return push(pack.at[1], full.at[me, core], ssem.at[1], rsem.at[1], (peer(1), c))

    def far_copy(k, p):
        spot = full.at[peer(k), core, p]
        return push(spot, spot, fs.at[k], fr.at[k], (me, far))

    def near_copy(k, side):
        spot = full.at[peer(k), side, plane]
        return push(spot, spot, ns.at[k], nr.at[k], (me, near))

    def near_pair(k, side):
        spot = full.at[peer(k), side]
        return push(spot, spot, ns.at[k], nr.at[k], (me, near))

    def relay_copy(k, side):
        spot = full.at[peer(k), side, oplane]
        return push(spot, spot, es.at[k], er.at[k], (me, near))

    def part_copy(k):
        return push(back.at[k, ocore], part.at[k], ps.at[k], pr.at[k], (me, near))

    def x_copy(k):
        return push(xbuf.at[k], xrecv.at[k], xs.at[k], xr.at[k], (me, far))

    def home_copy(k):
        return push(sendbuf.at[k], ret.at[k], hs.at[k], hr.at[k], (peer(k), c))

    fill(pack.at[1, plane], peer(1), c)
    fill(pack.at[1, oplane], peer(1), far)
    fill(pack.at[2, plane], peer(2), c)
    pl.semaphore_wait(barrier, n_sp - 1 + 2)
    out_pair().start()

    def send_out(k, carry):
        @pl.when(k < n_sp)
        def _():
            fill(pack.at[k, plane], peer(k), c)

        out_copy(k - 1).start()
        return carry

    lax.fori_loop(3, n_sp + 1, send_out, 0)
    fill(full.at[me, core, plane], me, c)
    fill(full.at[me, core, oplane], me, far)

    lower = jnp.where(row >= col, 1.0, 0.0)
    running = lax.dot_general(
        lower, log_decay[...], (((1,), (0,)), ((), ())), preferred_element_type=F32,
        precision=lax.Precision.HIGHEST,
    )
    for h in range(heads):
        totb[h] = jnp.broadcast_to(running[tokens - 1 : tokens, h : h + 1], totb.shape[1:])
    near_pair(0, core).start()
    start_cos, start_sin = cos_s[pl.ds(me, 1), :], sin_s[pl.ds(me, 1), :]
    cosines = start_cos * cos_t[...] - start_sin * sin_t[...]
    sines = start_sin * cos_t[...] + start_cos * sin_t[...]
    cosb[...] = cosines
    sinb[...] = sines
    swap_tot = push(totb, toto, tsem.at[0], tsem.at[1], (other, c))
    swap_tot.start()
    rows_of = kd // SPLIT
    for h in range(heads):
        x = queries[:, h * kd : (h + 1) * kd].astype(F32)
        qr[h] = (x * cosines + swapped(x) * sines).astype(BF16)
        x = keys[:, h * kd : (h + 1) * kd].astype(F32)
        key = (x * cosines + swapped(x) * sines) * scale
        kr[h] = key.astype(BF16)
        run = running[:, h : h + 1]
        left = jnp.exp(running[tokens - 1 : tokens, h : h + 1] - run)
        dec[h] = jnp.exp(run)
        rem_[h] = left
        state = dot((key * left).astype(BF16), values[:, h * vd : (h + 1) * vd], 0, 0)
        for s in range(SPLIT):
            inner[h * SPLIT + s] = state[s * rows_of : (s + 1) * rows_of]
        spread_run = jnp.broadcast_to(run, (tokens, tokens))
        difference = spread_run - spread_run.T
        causal = row >= col
        mask[h] = jnp.where(causal, jnp.exp(jnp.where(causal, difference, 0.0)), 0.0)
    totals = (totb, toto)
    past = Scan(True, n_sp, me, c, (fzin, fzout, fmin, fmout), fsem, totals, heads)
    coming = Scan(False, n_sp, me, c, (bzin, bzout, bmin, bmout), bsem, totals, heads)
    past.clear()
    coming.clear()
    for cp in loads:
        cp.wait()
    swap_tot.wait()

    def compute(k):
        src = peer(k)

        @pl.when(k < 2)
        def _():
            near_pair(k, ocore).wait_recv()

        @pl.when(k >= 2)
        def _():
            near_copy(k, ocore).wait_recv()
            relay_copy(k, ocore).wait_recv()

        pre = 0.0
        act_grad = 0.0
        for t in range(n_tp):
            band = pl.ds(t * q, q)
            spot = full.at[src, t % 2, t // 2]
            pre = pre + dot(spot[0], gu[band, :], 1, 0)
            act_grad = act_grad + dot(spot[1], dw[:, band], 1, 1)
        gate_pre = pre[:, :hid]
        up_pre = pre[:, hid:]
        gate_clip = jnp.minimum(gate_pre, CLAMP_LIMIT)
        up_clip = jnp.clip(up_pre, -CLAMP_LIMIT, CLAMP_LIMIT)
        sig = 1.0 / (1.0 + jnp.exp(-GATE_SLOPE * gate_clip))
        gated = gate_clip * sig
        act[src] = (gated * (up_clip + 1.0)).astype(BF16)
        slope = sig + GATE_SLOPE * gated * (1.0 - sig)
        gpg = jnp.where(gate_pre < CLAMP_LIMIT, act_grad * (up_clip + 1.0) * slope, 0.0)
        upg = jnp.where(jnp.abs(up_pre) < CLAMP_LIMIT, act_grad * gated, 0.0)
        both = jnp.concatenate([gpg, upg], axis=1).astype(BF16)
        gug[src] = both
        for t in range(n_tp):
            back[k, t % 2, t // 2] = dot(both, gu[pl.ds(t * q, q), :], 1, 1).astype(BF16)
        part_copy(k).start()

    def first(k):
        part_copy(k).wait_recv()
        xbuf[k] = (back[k, core, oplane].astype(F32) + part[k, oplane].astype(F32)).astype(BF16)
        x_copy(k).start()

    def second(k):
        x_copy(k).wait_recv()
        total = (
            back[k, core, plane].astype(F32) + part[k, plane].astype(F32) + xrecv[k].astype(F32)
        ).astype(BF16)

        @pl.when(k == 0)
        def _():
            ret[0] = total

        @pl.when(k > 0)
        def _():
            sendbuf[k] = total
            home_copy(k).start()

    def local_retention():
        for h in range(heads):
            score = dot(qr[h], kr[h], 1, 1) * mask[h]
            wts[h] = score.astype(BF16)
            normed_f[:, h * vd : (h + 1) * vd] = dot(
                wts[h], values[:, h * vd : (h + 1) * vd], 1, 0
            )

    def step(n, carry):
        @pl.when(n == 1)
        def _():
            push(pack.at[1], full.at[peer(1), core], ssem.at[1], rsem.at[1], (me, far)).wait_recv()
            near_pair(1, core).start()

        @pl.when((n >= 2) & (n < n_sp))
        def _():
            spot = full.at[peer(n), core, plane]
            push(spot, spot, ssem.at[n], rsem.at[n], (me, far)).wait_recv()
            far_copy(n, plane).start()
            near_copy(n, core).start()

        @pl.when((n >= 3) & (n <= n_sp))
        def _():
            far_copy(n - 1, oplane).wait_recv()
            relay_copy(n - 1, core).start()

        @pl.when(n == past.slot)
        def _():
            past.step(inner)

        @pl.when(n == 1)
        def _():
            local_retention()

        @pl.when((n >= 2) & (n < n_sp + 2))
        def _():
            compute(n - 2)

        @pl.when((n >= 3) & (n < n_sp + 3))
        def _():
            first(n - 3)

        @pl.when((n >= 4) & (n < n_sp + 4))
        def _():
            second(n - 4)

        return carry

    lax.fori_loop(0, n_sp + 4, step, 0)

    for j in range(heads * SPLIT):
        incoming[j // SPLIT, pl.ds((j % SPLIT) * rows_of, rows_of), :] = past.result(j)
    for h in range(heads):
        band = slice(h * vd, (h + 1) * vd)
        kept = normed_f[:, band] + dec[h] * dot(qr[h], incoming[h], 1, 0)
        inverse = lax.rsqrt(jnp.mean(kept * kept, axis=1, keepdims=True) + EPSILON)
        inv[h] = inverse
        normed_f[:, band] = kept * inverse
        normed_own[:, band] = (kept * inverse).astype(BF16)
    normed_all[me] = normed_own[...]
    spread = Chain(normed_own, normed_all, n_sp, me, c, chain_sem, (0, 1))

    def arrive(k, carry):
        push(sendbuf.at[k], ret.at[k], hs.at[k], hr.at[k], (me, far)).wait_recv()
        return carry

    lax.fori_loop(1, n_sp, arrive, 0)

    def combine(k, total):
        return total + dot(pick[peer(k)], ret[k], 0, 0)

    mine = resid.at[core, plane]
    total = lax.fori_loop(0, n_sp, combine, og[:, cols(c)].astype(F32))
    resid[core, plane] = total.astype(BF16)
    to_far = push(mine, mine, gs.at[0], gr.at[0], (me, far))
    to_near = push(mine, mine, gs.at[1], gr.at[1], (me, near))
    to_far.start()
    to_near.start()
    spread.start()
    spot = resid.at[core, oplane]
    push(spot, spot, gs.at[0], gr.at[0], (me, far)).wait_recv()
    onward = push(spot, spot, gs.at[2], gr.at[2], (me, near))
    onward.start()
    for s, p in ((1, plane), (2, oplane)):
        spot = resid.at[ocore, p]
        push(spot, spot, gs.at[s], gr.at[s], (me, near)).wait_recv()

    half = tokens // 2
    group = rcols.shape[3]
    per_quarter = q // group
    per_group = group * n_sp // (q * n_tp)

    def band_of(index):
        g = index // per_group
        quarter = g // per_quarter
        return resid.at[
            lax.rem(quarter, 2), quarter // 2, pl.ds(core * half, half),
            pl.ds(pl.multiple_of(lax.rem(g, per_quarter) * group, 128), group),
        ]

    def col_copy(k):
        return push(band_of(peer(k)), rcols.at[me, core], cs.at[k], cr.at[k], (peer(k), c))

    def col_near(k, side):
        spot = rcols.at[peer(k), side]
        return push(spot, spot, ds.at[k], dr.at[k], (me, near))

    def send_cols(k, carry):
        col_copy(k).start()
        return carry

    lax.fori_loop(1, n_sp, send_cols, 0)
    for side in range(2):
        g = me // per_group
        quarter = g // per_quarter
        rcols[me, side] = resid[
            lax.rem(quarter, 2), quarter // 2, side * half : (side + 1) * half,
            pl.ds(pl.multiple_of(lax.rem(g, per_quarter) * group, 128), group),
        ]
    normed_grad = 0.0
    for t in range(n_tp):
        normed_grad = normed_grad + dot(
            resid[t % 2, t // 2], pw[pl.ds(t * q, q), :], 1, 0
        )
    grads = []
    for h in range(heads):
        band = slice(h * vd, (h + 1) * vd)
        ng = normed_grad[:, band]
        nf = normed_f[:, band]
        grad = inv[h] * (ng - nf * jnp.mean(ng * nf, axis=1, keepdims=True))
        grad_bf = grad.astype(BF16)
        grads.append(grad_bf)
        turned = (qr[h].astype(F32) * dec[h]).astype(BF16)
        state = dot(turned, grad_bf, 0, 0)
        for s in range(SPLIT):
            inner_g[h * SPLIT + s] = state[s * rows_of : (s + 1) * rows_of]

    def weights_grad(t):
        x = flat(full[:, lax.rem(t, 2), t // 2, 0])
        g = flat(full[:, lax.rem(t, 2), t // 2, 1])
        both = dot(x, flat(gug[...]), 0, 0).astype(BF16)
        gout[cols(t), :] = both[:, :hid]
        uout[cols(t), :] = both[:, hid:]
        dout[:, cols(t)] = dot(flat(act[...]), g, 0, 0).astype(BF16)

    def late(s, carry):
        @pl.when(s == coming.slot)
        def _():
            coming.step(inner_g)

        @pl.when(s < n_tp)
        def _():
            weights_grad(s)

        return carry

    lax.fori_loop(0, max(n_sp // 2, n_tp), late, 0)
    stores = [
        pltpu.make_async_copy(gout, gate_o.at[0], osem.at[0]),
        pltpu.make_async_copy(uout, up_o.at[0], osem.at[1]),
        pltpu.make_async_copy(dout, down_o.at[0], osem.at[2]),
    ]
    for cp in stores:
        cp.start()
    for d in range(1, n_sp // 2):
        spread.step(d)

    def relay_cols(k, carry):
        spot = rcols.at[peer(k), core]
        push(spot, spot, cs.at[k], cr.at[k], (me, far)).wait_recv()
        col_near(k, core).start()
        return carry

    lax.fori_loop(1, n_sp, relay_cols, 0)

    def unturn(x):
        return x * cosb[...] - swapped(x) * sinb[...]

    partial = []
    for h in range(heads):
        band = slice(h * vd, (h + 1) * vd)
        score = (dot(grads[h], values[:, band], 1, 1) * mask[h]).astype(BF16)
        qp = dot(score, kr[h], 1, 0) + dec[h] * dot(grads[h], incoming[h], 1, 1)
        query_o[:, h * kd : (h + 1) * kd] = unturn(qp).astype(BF16)
        partial.append((dot(score, qr[h], 0, 0), dot(wts[h], grads[h], 0, 0)))

    def near_cols(k, carry):
        col_near(k, ocore).wait_recv()
        return carry

    lax.fori_loop(1, n_sp, near_cols, 0)
    spread.finish()
    columns = rcols[...].reshape(n_sp * tokens, group)
    everyone = normed_all[...].reshape(n_sp * tokens, heads * vd)
    proj[...] = dot(columns, everyone, 0, 0)
    width = proj_o.shape[0]
    proj_o[...] = proj[pl.ds(pl.multiple_of(lax.rem(me, per_group) * width, 8), width), :]

    future = [coming.result(j) for j in range(heads * SPLIT)]
    for h in range(heads):
        band = slice(h * vd, (h + 1) * vd)
        key_part, value_part = partial[h]
        later = jnp.concatenate(future[h * SPLIT : (h + 1) * SPLIT], axis=0)
        kp = key_part + rem_[h] * dot(values[:, band], later, 1, 1)
        key_o[:, h * kd : (h + 1) * kd] = (unturn(kp) * scale).astype(BF16)
        value_o[:, band] = (value_part + rem_[h] * dot(kr[h], later, 1, 0)).astype(BF16)

    for cp in (to_far, to_near, onward):
        cp.wait_send()
    past.finish()
    coming.finish()

    def drain(k, carry):
        part_copy(k).wait_send()
        x_copy(k).wait_send()

        @pl.when(k < 2)
        def _():
            near_pair(k, core).wait_send()

        @pl.when(k == 1)
        def _():
            out_pair().wait_send()

        @pl.when(k >= 2)
        def _():
            out_copy(k).wait_send()
            far_copy(k, plane).wait_send()
            near_copy(k, core).wait_send()
            relay_copy(k, core).wait_send()

        @pl.when(k > 0)
        def _():
            home_copy(k).wait_send()
            col_copy(k).wait_send()
            col_near(k, core).wait_send()

        return carry

    lax.fori_loop(0, n_sp, drain, 0)
    for cp in stores:
        cp.wait()


def rotation_tables(n_sp, tokens, key_width):
    frequency = 10000.0 ** -np.linspace(0.0, 1.0, key_width // 2)
    frequency = np.repeat(frequency, 2)
    angle = np.arange(tokens)[:, None] * frequency[None, :]
    start = tokens * np.arange(n_sp)[:, None] * frequency[None, :]
    return [
        jnp.asarray(table.astype(np.float32))
        for table in (np.cos(angle), np.sin(angle), np.cos(start), np.sin(start))
    ]


def per_device(
    stream, out_grad, routes, route_weight, queries, key_vectors, value_vectors, log_decay,
    out_proj, gate_weight, up_weight, down_weight,
):
    n_sp = lax.axis_size("sp")
    n_tp = lax.axis_size("tp")
    tokens, width = stream.shape
    cap = 4 * tokens // n_sp
    q = width // n_tp
    heads, kd = queries.shape[1:]
    vd = value_vectors.shape[2]
    hid = gate_weight.shape[2]
    w = width // n_sp
    group = max(w, 128)
    count, rows_of = heads * SPLIT, kd // SPLIT
    vmem, dma = pltpu.VMEM, pltpu.SemaphoreType.DMA
    block = vmem((n_sp, cap, q), BF16)
    packet = vmem((count, rows_of, vd), BF16)
    tables = rotation_tables(n_sp, tokens, kd)
    outs = pl.pallas_call(
        functools.partial(whole_kernel, n_sp, n_tp, heads),
        out_shape=(
            jax.ShapeDtypeStruct(gate_weight.shape, BF16),
            jax.ShapeDtypeStruct(up_weight.shape, BF16),
            jax.ShapeDtypeStruct(down_weight.shape, BF16),
            jax.ShapeDtypeStruct((w, heads * vd), F32),
            jax.ShapeDtypeStruct((tokens, heads * kd), BF16),
            jax.ShapeDtypeStruct((tokens, heads * kd), BF16),
            jax.ShapeDtypeStruct((tokens, heads * vd), BF16),
        ),
        in_specs=vmem_specs(12) + any_specs(4),
        out_specs=tuple(any_specs(3) + vmem_specs(4)),
        scratch_shapes=[
            vmem((n_sp, 2, 2, 2, cap, q), BF16),
            vmem((n_sp, 2, 2, cap, q), BF16),
            vmem((width, 2 * hid), BF16),
            vmem((hid, width), BF16),
            vmem((width, heads * vd), BF16),
            vmem((n_sp, cap, hid), BF16),
            vmem((n_sp, cap, 2 * hid), BF16),
            vmem((n_sp, 2, 2, cap, q), BF16),
            vmem((n_sp, 2, cap, q), BF16),
            block, block, block, block,
            vmem((width, hid), BF16),
            vmem((width, hid), BF16),
            vmem((hid, width), BF16),
            vmem((n_sp, cap, tokens), BF16),
            vmem((n_sp, cap, 1), F32),
            vmem((n_sp, tokens), F32),
            vmem((n_sp, tokens), F32),
            vmem((2, 2, tokens, q), BF16),
            vmem((n_sp, 2, tokens // 2, group), BF16),
            vmem((tokens, heads * vd), BF16),
            vmem((n_sp, tokens, heads * vd), BF16),
            vmem((tokens, heads * vd), F32),
            vmem((heads, tokens, 1), F32),
            vmem((heads, tokens, 1), F32),
            vmem((heads, tokens, 1), F32),
            vmem((heads, tokens, tokens), F32),
            vmem((heads, tokens, tokens), BF16),
            vmem((heads, tokens, kd), BF16),
            vmem((heads, tokens, kd), BF16),
            vmem((tokens, kd), F32),
            vmem((tokens, kd), F32),
            vmem((heads, 8, 128), F32),
            vmem((heads, 8, 128), F32),
            vmem((count, rows_of, vd), F32),
            vmem((count, rows_of, vd), F32),
            vmem((heads, kd, vd), BF16),
            vmem((group, heads * vd), F32),
        ]
        + [packet] * 8
        + [dma((4,)), dma((3,)), dma((2,))]
        + [dma((n_sp,))] * 14
        + [dma((3,))] * 2
        + [dma((n_sp,))] * 4
        + [dma((count,))] * 8
        + [dma((2, n_sp // 2))] * 4,
        compiler_params=pltpu.CompilerParams(
            collective_id=0, has_side_effects=True, vmem_limit_bytes=60 * 2**20
        ),
        name="whole",
    )(
        stream, out_grad, routes.T, route_weight.T, queries.reshape(tokens, heads * kd),
        key_vectors.reshape(tokens, heads * kd), value_vectors.reshape(tokens, heads * vd),
        log_decay, *tables, gate_weight, up_weight, down_weight, out_proj,
    )
    gate, up, down, proj, query, key, value = outs
    return (
        gate, up, down, proj, query.reshape(queries.shape), key.reshape(queries.shape),
        value.reshape(value_vectors.shape),
    )


def solution(mesh):
    in_specs = (
        P("sp", None),
        P("sp", None),
        P("sp", None),
        P("sp", None),
        P("sp", "tp", None),
        P("sp", "tp", None),
        P("sp", "tp", None),
        P("sp", "tp"),
        P(None, "tp"),
        P("sp", None, "tp"),
        P("sp", None, "tp"),
        P("sp", "tp", None),
    )
    out_specs = (
        P("sp", None, "tp"),
        P("sp", None, "tp"),
        P("sp", "tp", None),
        P("sp", "tp"),
        P("sp", "tp", None),
        P("sp", "tp", None),
        P("sp", "tp", None),
    )
    return jax.shard_map(
        per_device, mesh=mesh, in_specs=in_specs, out_specs=out_specs, check_vma=False
    )
```

```python
import functools

import jax
import jax.numpy as jnp
import numpy as np
from jax import lax
from jax.experimental import pallas as pl
from jax.experimental.pallas import tpu as pltpu
from jax.sharding import PartitionSpec as P

CLAMP_LIMIT = 7.0
GATE_SLOPE = 1.702
EPSILON = 1e-06
F32 = jnp.float32
BF16 = jnp.bfloat16
MESH = pl.DeviceIdType.MESH
SPLIT = 2


def any_specs(count):
    return [pl.BlockSpec(memory_space=pl.ANY)] * count


def vmem_specs(count):
    return [pl.BlockSpec(memory_space=pltpu.VMEM)] * count


def push(src, dst, send_sem, recv_sem, device):
    return pltpu.make_async_remote_copy(
        src_ref=src,
        dst_ref=dst,
        send_sem=send_sem,
        recv_sem=recv_sem,
        device_id=device,
        device_id_type=MESH,
    )


class Chain:
    def __init__(self, src, out, n_sp, me, c, sems, ways):
        self.src, self.out, self.me, self.c = src, out, me, c
        self.pairs, self.ways = n_sp // 2, ways
        self.pair = me // 2
        self.other = me + 1 - 2 * lax.rem(me, 2)
        self.zs, self.zr, self.ys, self.yr = sems

    def has(self, d, way):
        return self.pair >= d if way == 0 else self.pair + d < self.pairs

    def room(self, way):
        return self.pair + 1 < self.pairs if way == 0 else self.pair >= 1

    def spot(self, base, d, way):
        return self.out.at[base - 2 * d if way == 0 else base + 2 * d]

    def along(self, d, way):
        spot = self.spot(self.me, d, way)
        return push(
            self.src if d == 0 else spot, spot, self.zs.at[way, d], self.zr.at[way, d + 1],
            (self.me + 2 if way == 0 else self.me - 2, self.c),
        )

    def across(self, d, way):
        spot = self.spot(self.me, d, way)
        return push(
            self.src if d == 0 else spot, spot, self.ys.at[way, d], self.yr.at[way, d],
            (self.other, self.c),
        )

    def each(self, d, act):
        for way in self.ways:

            @pl.when(self.has(d, way))
            def _():
                if d < self.pairs - 1:

                    @pl.when(self.room(way))
                    def _():
                        act(self.along(d, way))

                if d > 0 or way == self.ways[0]:
                    act(self.across(d, way))

    def start(self):
        self.each(0, lambda cp: cp.start())

    def step(self, d):
        for way in self.ways:

            @pl.when(self.has(d, way))
            def _():
                spot = self.spot(self.me, d, way)
                push(
                    spot, spot, self.zs.at[way, d], self.zr.at[way, d], (self.other, self.c)
                ).wait_recv()

        self.each(d, lambda cp: cp.start())

    def finish(self):
        for d in range(self.pairs):
            for way in self.ways:
                if d == 0 and way != self.ways[0]:
                    continue

                @pl.when(self.has(d, way))
                def _():
                    spot = self.spot(self.other, d, way)
                    push(
                        spot, spot, self.ys.at[way, d], self.yr.at[way, d], (self.other, self.c)
                    ).wait_recv()

            self.each(d, lambda cp: cp.wait_send())


class Scan:
    def __init__(self, forward, n_sp, me, c, bufs, sems, totals, heads):
        self.forward, self.me, self.c = forward, me, c
        self.zin, self.zout, self.min, self.mout = bufs
        self.zs, self.zr, self.ms, self.mr = sems
        self.own_tot, self.other_tot = totals
        pairs = n_sp // 2
        pair = me // 2
        parity = lax.rem(me, 2)
        self.other = me + 1 - 2 * parity
        self.prev = pair > 0 if forward else pair + 1 < pairs
        self.next = pair + 1 < pairs if forward else pair > 0
        self.ahead = me + 2 if forward else me - 2
        self.slot = pair if forward else pairs - 1 - pair
        self.inside = jnp.where(parity == (0 if forward else 1), 1.0, 0.0)
        self.count = heads * SPLIT

    def z_copy(self, j):
        return push(
            self.zout.at[j], self.zin.at[j], self.zs.at[j], self.zr.at[j], (self.ahead, self.c)
        )

    def m_copy(self, j):
        return push(
            self.mout.at[j], self.min.at[j], self.ms.at[j], self.mr.at[j], (self.other, self.c)
        )

    def clear(self):
        @pl.when(jnp.logical_not(self.prev))
        def _():
            self.zin[...] = jnp.zeros_like(self.zin)

    def decays(self, j):
        h = j // SPLIT
        return jnp.exp(self.own_tot[h, 0:1, 0:1]), jnp.exp(self.other_tot[h, 0:1, 0:1])

    def step(self, own):
        s = self.inside
        for j in range(self.count):
            mine, others = self.decays(j)

            @pl.when(self.prev)
            def _():
                self.z_copy(j).wait_recv()

            z = self.zin[j].astype(F32)
            i = own[j]
            self.zout[j] = (mine * others * z + (s * others + (1.0 - s)) * i).astype(BF16)

            @pl.when(self.next)
            def _():
                self.z_copy(j).start()

            self.mout[j] = ((s * mine + (1.0 - s)) * z + s * i).astype(BF16)
            self.m_copy(j).start()

    def result(self, j):
        s = self.inside
        others = self.decays(j)[1]
        self.m_copy(j).wait_recv()
        z = self.zin[j].astype(F32)
        return (self.min[j].astype(F32) + (s + (1.0 - s) * others) * z).astype(BF16)

    def finish(self):
        for j in range(self.count):

            @pl.when(self.next)
            def _():
                self.z_copy(j).wait_send()

            self.m_copy(j).wait_send()


def dot(a, b, da, db):
    return lax.dot_general(a, b, (((da,), (db,)), ((), ())), preferred_element_type=F32)


def flat(block):
    n, cap, q = block.shape
    if cap % 16 == 0:
        return block.reshape(n * cap, q)
    return block.astype(F32).reshape(n * cap, q).astype(BF16)


def swapped(x):
    width = x.shape[1]
    even = lax.rem(lax.broadcasted_iota(jnp.int32, x.shape, 1), 2) == 0
    return jnp.where(even, -pltpu.roll(x, width - 1, 1), pltpu.roll(x, 1, 1))


def whole_kernel(
    n_sp, n_tp, heads,
    stream, og, routes, route_w, queries, keys, values, log_decay, cos_t, sin_t, cos_s, sin_s,
    gate_w, up_w, down_w, proj_w,
    gate_o, up_o, down_o, proj_o, query_o, key_o, value_o,
    full, pack, gu, dw, pw, act, gug, back, part, xbuf, xrecv, sendbuf, ret,
    pick, wcol, slotmap, weight_map, resid, rcols, normed_own, normed_all, normed_f, inv, dec, rem_,
    mask, wts, qr, kr, val, cosb, sinb, totb, toto, inner, inner_g, incoming, proj,
    fzin, fzout, fmin, fmout, bzin, bzout, bmin, bmout,
    wsem, tsem, ssem, rsem, fs, fr, ns, nr, es, er, ps, pr, xs, xr, hs, hr, gs, gr,
    cs, cr, ds, dr, *more,
):
    fsem, bsem, chain_sem = more[0:4], more[4:8], more[8:12]
    me = lax.axis_index("sp")
    c = lax.axis_index("tp")
    core, plane = lax.rem(c, 2), c // 2
    ocore, oplane = 1 - core, 1 - plane
    far = lax.rem(c + n_tp // 2, n_tp)
    near = c + 1 - 2 * core
    other = me + 1 - 2 * lax.rem(me, 2)
    cap, q = full.shape[4:]
    hid = dw.shape[0]
    tokens = stream.shape[0]
    kd = cos_t.shape[1]
    vd = values.shape[2]
    scale = kd ** (-0.5)
    bits = [1 << b for b in range((n_sp - 1).bit_length())]

    def peer(k):
        out = 0
        for b in bits:
            out = out + b * lax.rem(me // b + k // b, 2)
        return out

    loads = [
        pltpu.make_async_copy(gate_w.at[0], gu.at[:, pl.ds(0, hid)], wsem.at[0]),
        pltpu.make_async_copy(up_w.at[0], gu.at[:, pl.ds(hid, hid)], wsem.at[1]),
        pltpu.make_async_copy(down_w.at[0], dw, wsem.at[2]),
        pltpu.make_async_copy(proj_w, pw, wsem.at[3]),
    ]
    for cp in loads:
        cp.start()
    barrier = pltpu.get_barrier_semaphore()

    def hello(k, carry):
        pl.semaphore_signal(barrier, inc=1, device_id=(peer(k), c), device_id_type=MESH)
        return carry

    lax.fori_loop(1, n_sp, hello, 0)
    for t in (far, near):
        pl.semaphore_signal(barrier, inc=1, device_id=(me, t), device_id_type=MESH)

    def cols(index):
        return pl.ds(pl.multiple_of(index * q, 128), q)

    expert = lax.broadcasted_iota(jnp.int32, (n_sp, tokens), 0)
    first_of = expert == routes[0:1, :]
    second_of = expert == routes[1:2, :]
    chosen = first_of | second_of
    weight_map[...] = jnp.where(first_of, route_w[0:1, :], 0.0) + jnp.where(
        second_of, route_w[1:2, :], 0.0
    )
    row = lax.broadcasted_iota(jnp.int32, (tokens, tokens), 0)
    col = lax.broadcasted_iota(jnp.int32, (tokens, tokens), 1)
    earlier = jnp.where(row < col, 1.0, 0.0).astype(BF16)
    before = dot(jnp.where(chosen, 1.0, 0.0).astype(BF16), earlier, 1, 0)
    slotmap[...] = jnp.where(chosen, before, -1.0)
    place = lax.broadcasted_iota(jnp.int32, (cap, tokens), 0).astype(F32)
    for e in range(n_sp):
        hit = jnp.where(slotmap[e : e + 1, :] == place, 1.0, 0.0)
        pick[e] = hit.astype(BF16)
        wcol[e] = jnp.sum(hit * weight_map[e : e + 1, :], axis=1, keepdims=True)

    def fill(spot, e, index):
        rows = dot(pick[e], stream[:, cols(index)], 1, 0)
        grads = wcol[e] * dot(pick[e], og[:, cols(index)], 1, 0)
        spot[0] = rows.astype(BF16)
        spot[1] = grads.astype(BF16)

    def out_copy(k):
        return push(
            pack.at[k, plane], full.at[me, core, plane], ssem.at[k], rsem.at[k], (peer(k), c)
        )

    def out_pair():
        return push(pack.at[1], full.at[me, core], ssem.at[1], rsem.at[1], (peer(1), c))

    def far_copy(k, p):
        spot = full.at[peer(k), core, p]
        return push(spot, spot, fs.at[k], fr.at[k], (me, far))

    def near_copy(k, side):
        spot = full.at[peer(k), side, plane]
        return push(spot, spot, ns.at[k], nr.at[k], (me, near))

    def near_pair(k, side):
        spot = full.at[peer(k), side]
        return push(spot, spot, ns.at[k], nr.at[k], (me, near))

    def relay_copy(k, side):
        spot = full.at[peer(k), side, oplane]
        return push(spot, spot, es.at[k], er.at[k], (me, near))

    def part_copy(k):
        return push(back.at[k, ocore], part.at[k], ps.at[k], pr.at[k], (me, near))

    def x_copy(k):
        return push(xbuf.at[k], xrecv.at[k], xs.at[k], xr.at[k], (me, far))

    def home_copy(k):
        return push(sendbuf.at[k], ret.at[k], hs.at[k], hr.at[k], (peer(k), c))

    fill(pack.at[1, plane], peer(1), c)
    fill(pack.at[1, oplane], peer(1), far)
    fill(pack.at[2, plane], peer(2), c)
    running = lax.dot_general(
        log_decay[...], jnp.where(row <= col, 1.0, 0.0), (((1,), (0,)), ((), ())),
        preferred_element_type=F32, precision=lax.Precision.HIGHEST,
    )
    for h in range(heads):
        totb[h] = jnp.broadcast_to(running[h : h + 1, tokens - 1 : tokens], totb.shape[1:])
    start_cos, start_sin = cos_s[pl.ds(me, 1), :], sin_s[pl.ds(me, 1), :]
    cosines = start_cos * cos_t[...] - start_sin * sin_t[...]
    sines = start_sin * cos_t[...] + start_cos * sin_t[...]
    cosb[...] = cosines
    sinb[...] = sines
    rows_of = kd // SPLIT
    for h in range(heads):
        x = queries[:, h, :].astype(F32)
        qr[h] = (x * cosines + swapped(x) * sines).astype(BF16)
        x = keys[:, h, :].astype(F32)
        key = (x * cosines + swapped(x) * sines) * scale
        kr[h] = key.astype(BF16)
        val[h] = values[:, h, :]
        along = jnp.broadcast_to(running[h : h + 1, :], (tokens, tokens))
        down = along.T
        run = down[:, 0:1]
        left = jnp.exp(running[h : h + 1, tokens - 1 : tokens] - run)
        dec[h] = jnp.exp(run)
        rem_[h] = left
        state = dot((key * left).astype(BF16), val[h], 0, 0)
        for s in range(SPLIT):
            inner[h * SPLIT + s] = state[s * rows_of : (s + 1) * rows_of]
        causal = row >= col
        mask[h] = jnp.where(causal, jnp.exp(jnp.where(causal, down - along, 0.0)), 0.0)
    totals = (totb, toto)
    past = Scan(True, n_sp, me, c, (fzin, fzout, fmin, fmout), fsem, totals, heads)
    coming = Scan(False, n_sp, me, c, (bzin, bzout, bmin, bmout), bsem, totals, heads)
    past.clear()
    coming.clear()
    pairs = n_sp // 2
    pace = (n_sp + 4) // pairs
    early = n_sp * 3 // 4
    pl.semaphore_wait(barrier, n_sp - 1 + 2)
    swap_tot = push(totb, toto, tsem.at[0], tsem.at[1], (other, c))
    swap_tot.start()
    out_pair().start()
    out_copy(2).start()
    fill(full.at[me, core, plane], me, c)
    fill(full.at[me, core, oplane], me, far)

    def fill_rest(k, carry):
        fill(pack.at[k, plane], peer(k), c)
        return carry

    lax.fori_loop(3, n_sp, fill_rest, 0)
    near_pair(0, core).start()
    swap_tot.wait()

    @pl.when(past.slot == 0)
    def _():
        past.step(inner)

    def send_out(k, carry):
        out_copy(k).start()
        return carry

    lax.fori_loop(3, early, send_out, 0)
    for cp in loads:
        cp.wait()

    def compute(k):
        src = peer(k)

        @pl.when(k < 2)
        def _():
            near_pair(k, ocore).wait_recv()

        @pl.when(k >= 2)
        def _():
            near_copy(k, ocore).wait_recv()
            relay_copy(k, ocore).wait_recv()

        pre = 0.0
        act_grad = 0.0
        for t in range(n_tp):
            band = pl.ds(t * q, q)
            spot = full.at[src, t % 2, t // 2]
            pre = pre + dot(spot[0], gu[band, :], 1, 0)
            act_grad = act_grad + dot(spot[1], dw[:, band], 1, 1)
        gate_pre = pre[:, :hid]
        up_pre = pre[:, hid:]
        gate_clip = jnp.minimum(gate_pre, CLAMP_LIMIT)
        up_clip = jnp.clip(up_pre, -CLAMP_LIMIT, CLAMP_LIMIT)
        sig = 1.0 / (1.0 + jnp.exp(-GATE_SLOPE * gate_clip))
        gated = gate_clip * sig
        act[src] = (gated * (up_clip + 1.0)).astype(BF16)
        slope = sig + GATE_SLOPE * gated * (1.0 - sig)
        gpg = jnp.where(gate_pre < CLAMP_LIMIT, act_grad * (up_clip + 1.0) * slope, 0.0)
        upg = jnp.where(jnp.abs(up_pre) < CLAMP_LIMIT, act_grad * gated, 0.0)
        both = jnp.concatenate([gpg, upg], axis=1).astype(BF16)
        gug[src] = both
        for t in range(n_tp):
            back[k, t % 2, t // 2] = dot(both, gu[pl.ds(t * q, q), :], 1, 1).astype(BF16)
        part_copy(k).start()

    def first(k):
        part_copy(k).wait_recv()
        xbuf[k] = (back[k, core, oplane].astype(F32) + part[k, oplane].astype(F32)).astype(BF16)
        x_copy(k).start()

    def second(k):
        x_copy(k).wait_recv()
        total = (
            back[k, core, plane].astype(F32) + part[k, plane].astype(F32) + xrecv[k].astype(F32)
        ).astype(BF16)

        @pl.when(k == 0)
        def _():
            ret[0] = total

        @pl.when(k > 0)
        def _():
            sendbuf[k] = total
            home_copy(k).start()

    def local_retention():
        for h in range(heads):
            score = dot(qr[h], kr[h], 1, 1) * mask[h]
            wts[h] = score.astype(BF16)
            normed_f[:, h * vd : (h + 1) * vd] = dot(wts[h], val[h], 1, 0)

    def turn_of(n):
        return jnp.where((n >= 1) & (n <= 4), 1 + lax.rem(n, 4), n)

    compute(0)
    local_retention()

    def step(n, carry):
        k = turn_of(n)

        @pl.when((n < n_sp) & (k == 1))
        def _():
            spot = full.at[peer(1), core]
            push(spot, spot, ssem.at[1], rsem.at[1], (me, far)).wait_recv()
            near_pair(1, core).start()

        @pl.when((n < n_sp) & (k > 1))
        def _():
            spot = full.at[peer(k), core, plane]
            push(spot, spot, ssem.at[k], rsem.at[k], (me, far)).wait_recv()
            far_copy(k, plane).start()
            near_copy(k, core).start()

        j = turn_of(n - 1)

        @pl.when((n <= n_sp) & (j > 1))
        def _():
            far_copy(j, oplane).wait_recv()
            relay_copy(j, core).start()

        @pl.when((n == past.slot * pace) & (past.slot > 0))
        def _():
            past.step(inner)

        @pl.when(n == pace)
        def _():
            lax.fori_loop(early, n_sp, send_out, 0)

        @pl.when(n == 1)
        def _():
            first(0)

        @pl.when(n == 2)
        def _():
            second(0)

        @pl.when((n >= 3) & (n < n_sp + 2))
        def _():
            compute(turn_of(n - 2))

        @pl.when((n >= 4) & (n < n_sp + 3))
        def _():
            first(turn_of(n - 3))

        @pl.when((n >= 5) & (n < n_sp + 4))
        def _():
            second(turn_of(n - 4))

        return carry

    lax.fori_loop(1, n_sp + 4, step, 0)

    for j in range(heads * SPLIT):
        incoming[j // SPLIT, pl.ds((j % SPLIT) * rows_of, rows_of), :] = past.result(j)
    for h in range(heads):
        band = slice(h * vd, (h + 1) * vd)
        kept = normed_f[:, band] + dec[h] * dot(qr[h], incoming[h], 1, 0)
        inverse = lax.rsqrt(jnp.mean(kept * kept, axis=1, keepdims=True) + EPSILON)
        inv[h] = inverse
        normed_f[:, band] = kept * inverse
        normed_own[:, band] = (kept * inverse).astype(BF16)
    normed_all[me] = normed_own[...]
    spread = Chain(normed_own, normed_all, n_sp, me, c, chain_sem, (0, 1))
    spread.start()

    def arrive(k, total):
        push(sendbuf.at[k], ret.at[k], hs.at[k], hr.at[k], (me, far)).wait_recv()
        return total + dot(pick[peer(k)], ret[k], 0, 0)

    total = og[:, cols(c)].astype(F32) + dot(pick[me], ret[0], 0, 0)
    total = lax.fori_loop(1, n_sp, arrive, total)
    half = tokens // 2
    resid[core, plane] = total.astype(BF16)

    def strip(side, p, i):
        return resid.at[side, p, pl.ds(i * half, half)]

    sent = []
    for i in range(2):
        mine = strip(core, plane, i)
        sent.append(push(mine, mine, gs.at[0, i], gr.at[0, i], (me, far)))
    for i in range(2):
        mine = strip(core, plane, i)
        sent.append(push(mine, mine, gs.at[1, i], gr.at[1, i], (me, near)))
    for cp in sent:
        cp.start()
    spread.step(1)

    def share(side, p):
        return dot(resid[side, p], pw[cols(2 * p + side), :], 1, 0)

    normed_grad = share(core, plane)
    for i in range(2):
        spot = strip(core, oplane, i)
        push(spot, spot, gs.at[0, i], gr.at[0, i], (me, far)).wait_recv()
        onward = push(spot, spot, gs.at[2, i], gr.at[2, i], (me, near))
        onward.start()
        sent.append(onward)
    normed_grad = normed_grad + share(core, oplane)
    for j, p in ((1, plane), (2, oplane)):
        for i in range(2):
            spot = strip(ocore, p, i)
            push(spot, spot, gs.at[j, i], gr.at[j, i], (me, near)).wait_recv()
        normed_grad = normed_grad + share(ocore, p)

    group = rcols.shape[3]
    per_quarter = q // group
    per_group = group * n_sp // (q * n_tp)

    def band_of(index):
        g = index // per_group
        quarter = g // per_quarter
        return resid.at[
            lax.rem(quarter, 2), quarter // 2, pl.ds(core * half, half),
            pl.ds(pl.multiple_of(lax.rem(g, per_quarter) * group, 128), group),
        ]

    def col_copy(k):
        return push(band_of(peer(k)), rcols.at[me, core], cs.at[k], cr.at[k], (peer(k), c))

    def col_near(k, side):
        spot = rcols.at[peer(k), side]
        return push(spot, spot, ds.at[k], dr.at[k], (me, near))

    def send_cols(k, carry):
        col_copy(k).start()
        return carry

    grads = []
    for h in range(heads):
        band = slice(h * vd, (h + 1) * vd)
        ng = normed_grad[:, band]
        nf = normed_f[:, band]
        grad = inv[h] * (ng - nf * jnp.mean(ng * nf, axis=1, keepdims=True))
        grad_bf = grad.astype(BF16)
        grads.append(grad_bf)
        turned = (qr[h].astype(F32) * dec[h]).astype(BF16)
        state = dot(turned, grad_bf, 0, 0)
        for s in range(SPLIT):
            inner_g[h * SPLIT + s] = state[s * rows_of : (s + 1) * rows_of]

    def weights_grad(t):
        x = flat(full[:, lax.rem(t, 2), t // 2, 0])
        g = flat(full[:, lax.rem(t, 2), t // 2, 1])
        both = dot(x, flat(gug[...]), 0, 0).astype(BF16)
        gate_o[0, cols(t), :] = both[:, :hid]
        up_o[0, cols(t), :] = both[:, hid:]
        down_o[0, :, cols(t)] = dot(flat(act[...]), g, 0, 0).astype(BF16)

    @pl.when(coming.slot == 0)
    def _():
        coming.step(inner_g)

    lax.fori_loop(1, n_sp, send_cols, 0)

    def late(s, carry):
        @pl.when((s == coming.slot) & (s > 0))
        def _():
            coming.step(inner_g)

        if pairs > 2:

            @pl.when(s == 1)
            def _():
                spread.step(2)

        @pl.when(s < n_tp)
        def _():
            weights_grad(s)

        return carry

    lax.fori_loop(0, max(pairs, n_tp), late, 0)
    for d in range(3, pairs):
        spread.step(d)
    for side in range(2):
        g = me // per_group
        quarter = g // per_quarter
        rcols[me, side] = resid[
            lax.rem(quarter, 2), quarter // 2, side * half : (side + 1) * half,
            pl.ds(pl.multiple_of(lax.rem(g, per_quarter) * group, 128), group),
        ]

    def relay_cols(k, carry):
        spot = rcols.at[peer(k), core]
        push(spot, spot, cs.at[k], cr.at[k], (me, far)).wait_recv()
        col_near(k, core).start()
        return carry

    lax.fori_loop(1, n_sp, relay_cols, 0)

    def unturn(x):
        return x * cosb[...] - swapped(x) * sinb[...]

    partial = []
    for h in range(heads):
        score = (dot(grads[h], val[h], 1, 1) * mask[h]).astype(BF16)
        qp = dot(score, kr[h], 1, 0) + dec[h] * dot(grads[h], incoming[h], 1, 1)
        query_o[:, h * kd : (h + 1) * kd] = unturn(qp).astype(BF16)
        partial.append((dot(score, qr[h], 0, 0), dot(wts[h], grads[h], 0, 0)))

    def near_cols(k, carry):
        col_near(k, ocore).wait_recv()
        return carry

    lax.fori_loop(1, n_sp, near_cols, 0)
    spread.finish()
    columns = rcols[...].reshape(n_sp * tokens, group)
    everyone = normed_all[...].reshape(n_sp * tokens, heads * vd)
    proj[...] = dot(columns, everyone, 0, 0)
    width = proj_o.shape[0]
    proj_o[...] = proj[pl.ds(pl.multiple_of(lax.rem(me, per_group) * width, 8), width), :]

    future = [coming.result(j) for j in range(heads * SPLIT)]
    for h in range(heads):
        band = slice(h * vd, (h + 1) * vd)
        key_part, value_part = partial[h]
        later = jnp.concatenate(future[h * SPLIT : (h + 1) * SPLIT], axis=0)
        kp = key_part + rem_[h] * dot(val[h], later, 1, 1)
        key_o[:, h * kd : (h + 1) * kd] = (unturn(kp) * scale).astype(BF16)
        value_o[:, band] = (value_part + rem_[h] * dot(kr[h], later, 1, 0)).astype(BF16)

    for cp in sent:
        cp.wait_send()
    past.finish()
    coming.finish()

    def drain(k, carry):
        part_copy(k).wait_send()
        x_copy(k).wait_send()

        @pl.when(k < 2)
        def _():
            near_pair(k, core).wait_send()

        @pl.when(k == 1)
        def _():
            out_pair().wait_send()

        @pl.when(k >= 2)
        def _():
            out_copy(k).wait_send()
            far_copy(k, plane).wait_send()
            near_copy(k, core).wait_send()
            relay_copy(k, core).wait_send()

        @pl.when(k > 0)
        def _():
            home_copy(k).wait_send()
            col_copy(k).wait_send()
            col_near(k, core).wait_send()

        return carry

    lax.fori_loop(0, n_sp, drain, 0)


def finish_kernel(
    gate, up, down, proj, query, key, value, gate_o, up_o, down_o, proj_o, query_o, key_o, value_o,
    sem,
):
    pairs = ((gate, gate_o), (up, up_o), (down, down_o), (proj, proj_o))
    stores = [pltpu.make_async_copy(a, b, sem.at[i]) for i, (a, b) in enumerate(pairs)]
    for cp in stores:
        cp.start()
    for a, b in ((query, query_o), (key, key_o), (value, value_o)):
        width = b.shape[2]
        for h in range(b.shape[1]):
            b[:, h, :] = a[:, h * width : (h + 1) * width]
    for cp in stores:
        cp.wait()


def rotation_tables(n_sp, tokens, key_width):
    frequency = 10000.0 ** -np.linspace(0.0, 1.0, key_width // 2)
    frequency = np.repeat(frequency, 2)
    angle = np.arange(tokens)[:, None] * frequency[None, :]
    start = tokens * np.arange(n_sp)[:, None] * frequency[None, :]
    return [
        jnp.asarray(table.astype(np.float32))
        for table in (np.cos(angle), np.sin(angle), np.cos(start), np.sin(start))
    ]


def per_device(
    stream, out_grad, routes, route_weight, queries, key_vectors, value_vectors, log_decay,
    out_proj, gate_weight, up_weight, down_weight,
):
    n_sp = lax.axis_size("sp")
    n_tp = lax.axis_size("tp")
    tokens, width = stream.shape
    cap = 4 * tokens // n_sp
    q = width // n_tp
    heads, kd = queries.shape[1:]
    vd = value_vectors.shape[2]
    hid = gate_weight.shape[2]
    w = width // n_sp
    group = max(w, 128)
    count, rows_of = heads * SPLIT, kd // SPLIT
    vmem, dma = pltpu.VMEM, pltpu.SemaphoreType.DMA
    block = vmem((n_sp, cap, q), BF16)
    packet = vmem((count, rows_of, vd), BF16)
    tables = rotation_tables(n_sp, tokens, kd)
    outs = pl.pallas_call(
        functools.partial(whole_kernel, n_sp, n_tp, heads),
        out_shape=(
            jax.ShapeDtypeStruct(gate_weight.shape, BF16),
            jax.ShapeDtypeStruct(up_weight.shape, BF16),
            jax.ShapeDtypeStruct(down_weight.shape, BF16),
            jax.ShapeDtypeStruct((w, heads * vd), F32),
            jax.ShapeDtypeStruct((tokens, heads * kd), BF16),
            jax.ShapeDtypeStruct((tokens, heads * kd), BF16),
            jax.ShapeDtypeStruct((tokens, heads * vd), BF16),
        ),
        in_specs=vmem_specs(12) + [pl.BlockSpec(memory_space=pltpu.HBM)] * 4,
        out_specs=tuple(vmem_specs(7)),
        scratch_shapes=[
            vmem((n_sp, 2, 2, 2, cap, q), BF16),
            vmem((n_sp, 2, 2, cap, q), BF16),
            vmem((width, 2 * hid), BF16),
            vmem((hid, width), BF16),
            vmem((width, heads * vd), BF16),
            vmem((n_sp, cap, hid), BF16),
            vmem((n_sp, cap, 2 * hid), BF16),
            vmem((n_sp, 2, 2, cap, q), BF16),
            vmem((n_sp, 2, cap, q), BF16),
            block, block, block, block,
            vmem((n_sp, cap, tokens), BF16),
            vmem((n_sp, cap, 1), F32),
            vmem((n_sp, tokens), F32),
            vmem((n_sp, tokens), F32),
            vmem((2, 2, tokens, q), BF16),
            vmem((n_sp, 2, tokens // 2, group), BF16),
            vmem((tokens, heads * vd), BF16),
            vmem((n_sp, tokens, heads * vd), BF16),
            vmem((tokens, heads * vd), F32),
            vmem((heads, tokens, 1), F32),
            vmem((heads, tokens, 1), F32),
            vmem((heads, tokens, 1), F32),
            vmem((heads, tokens, tokens), F32),
            vmem((heads, tokens, tokens), BF16),
            vmem((heads, tokens, kd), BF16),
            vmem((heads, tokens, kd), BF16),
            vmem((heads, tokens, vd), BF16),
            vmem((tokens, kd), F32),
            vmem((tokens, kd), F32),
            vmem((heads, 8, 128), F32),
            vmem((heads, 8, 128), F32),
            vmem((count, rows_of, vd), F32),
            vmem((count, rows_of, vd), F32),
            vmem((heads, kd, vd), BF16),
            vmem((group, heads * vd), F32),
        ]
        + [packet] * 8
        + [dma((4,)), dma((2,))]
        + [dma((n_sp,))] * 14
        + [dma((3, 2))] * 2
        + [dma((n_sp,))] * 4
        + [dma((count,))] * 8
        + [dma((2, n_sp // 2))] * 4,
        compiler_params=pltpu.CompilerParams(
            collective_id=0, has_side_effects=True, vmem_limit_bytes=48 * 2**20
        ),
        name="whole",
    )(
        stream, out_grad, routes.T, route_weight.T, queries, key_vectors, value_vectors,
        log_decay.T, *tables, gate_weight, up_weight, down_weight, out_proj,
    )
    shapes = [jax.ShapeDtypeStruct(x.shape, x.dtype) for x in outs[:4]] + [
        jax.ShapeDtypeStruct(x.shape, BF16) for x in (queries, key_vectors, value_vectors)
    ]
    return pl.pallas_call(
        finish_kernel,
        out_shape=tuple(shapes),
        in_specs=vmem_specs(7),
        out_specs=tuple(any_specs(4) + vmem_specs(3)),
        scratch_shapes=[dma((4,))],
        compiler_params=pltpu.CompilerParams(vmem_limit_bytes=16 * 2**20),
        name="finish",
    )(*outs)


def solution(mesh):
    in_specs = (
        P("sp", None),
        P("sp", None),
        P("sp", None),
        P("sp", None),
        P("sp", "tp", None),
        P("sp", "tp", None),
        P("sp", "tp", None),
        P("sp", "tp"),
        P(None, "tp"),
        P("sp", None, "tp"),
        P("sp", None, "tp"),
        P("sp", "tp", None),
    )
    out_specs = (
        P("sp", None, "tp"),
        P("sp", None, "tp"),
        P("sp", "tp", None),
        P("sp", "tp"),
        P("sp", "tp", None),
        P("sp", "tp", None),
        P("sp", "tp", None),
    )
    return jax.shard_map(
        per_device, mesh=mesh, in_specs=in_specs, out_specs=out_specs, check_vma=False
    )
```

```python
import functools

import jax
import jax.numpy as jnp
import numpy as np
from jax import lax
from jax.experimental import pallas as pl
from jax.experimental.pallas import tpu as pltpu
from jax.sharding import PartitionSpec as P

CLAMP_LIMIT = 7.0
GATE_SLOPE = 1.702
EPSILON = 1e-06
F32 = jnp.float32
BF16 = jnp.bfloat16
MESH = pl.DeviceIdType.MESH
SPLIT = 2


def any_specs(count):
    return [pl.BlockSpec(memory_space=pl.ANY)] * count


def vmem_specs(count):
    return [pl.BlockSpec(memory_space=pltpu.VMEM)] * count


def push(src, dst, send_sem, recv_sem, device):
    return pltpu.make_async_remote_copy(
        src_ref=src,
        dst_ref=dst,
        send_sem=send_sem,
        recv_sem=recv_sem,
        device_id=device,
        device_id_type=MESH,
    )


class Chain:
    def __init__(self, src, out, n_sp, me, c, sems, ways):
        self.src, self.out, self.me, self.c = src, out, me, c
        self.pairs, self.ways = n_sp // 2, ways
        self.pair = me // 2
        self.other = me + 1 - 2 * lax.rem(me, 2)
        self.zs, self.zr, self.ys, self.yr = sems

    def has(self, d, way):
        return self.pair >= d if way == 0 else self.pair + d < self.pairs

    def room(self, way):
        return self.pair + 1 < self.pairs if way == 0 else self.pair >= 1

    def spot(self, base, d, way):
        return self.out.at[base - 2 * d if way == 0 else base + 2 * d]

    def along(self, d, way):
        spot = self.spot(self.me, d, way)
        return push(
            self.src if d == 0 else spot, spot, self.zs.at[way, d], self.zr.at[way, d + 1],
            (self.me + 2 if way == 0 else self.me - 2, self.c),
        )

    def across(self, d, way):
        spot = self.spot(self.me, d, way)
        return push(
            self.src if d == 0 else spot, spot, self.ys.at[way, d], self.yr.at[way, d],
            (self.other, self.c),
        )

    def each(self, d, act):
        for way in self.ways:

            @pl.when(self.has(d, way))
            def _():
                if d < self.pairs - 1:

                    @pl.when(self.room(way))
                    def _():
                        act(self.along(d, way))

                if d > 0 or way == self.ways[0]:
                    act(self.across(d, way))

    def start(self):
        self.each(0, lambda cp: cp.start())

    def step(self, d):
        for way in self.ways:

            @pl.when(self.has(d, way))
            def _():
                spot = self.spot(self.me, d, way)
                push(
                    spot, spot, self.zs.at[way, d], self.zr.at[way, d], (self.other, self.c)
                ).wait_recv()

        self.each(d, lambda cp: cp.start())

    def finish(self):
        for d in range(self.pairs):
            for way in self.ways:
                if d == 0 and way != self.ways[0]:
                    continue

                @pl.when(self.has(d, way))
                def _():
                    spot = self.spot(self.other, d, way)
                    push(
                        spot, spot, self.ys.at[way, d], self.yr.at[way, d], (self.other, self.c)
                    ).wait_recv()

            self.each(d, lambda cp: cp.wait_send())


class Scan:
    def __init__(self, forward, n_sp, me, c, bufs, sems, totals, heads):
        self.forward, self.me, self.c = forward, me, c
        self.zin, self.zout, self.min, self.mout = bufs
        self.zs, self.zr, self.ms, self.mr = sems
        self.own_tot, self.other_tot = totals
        pairs = n_sp // 2
        pair = me // 2
        parity = lax.rem(me, 2)
        self.other = me + 1 - 2 * parity
        self.prev = pair > 0 if forward else pair + 1 < pairs
        self.next = pair + 1 < pairs if forward else pair > 0
        self.ahead = me + 2 if forward else me - 2
        self.slot = pair if forward else pairs - 1 - pair
        self.inside = jnp.where(parity == (0 if forward else 1), 1.0, 0.0)
        self.count = heads * SPLIT

    def z_copy(self, j):
        return push(
            self.zout.at[j], self.zin.at[j], self.zs.at[j], self.zr.at[j], (self.ahead, self.c)
        )

    def m_copy(self, j):
        return push(
            self.mout.at[j], self.min.at[j], self.ms.at[j], self.mr.at[j], (self.other, self.c)
        )

    def clear(self):
        @pl.when(jnp.logical_not(self.prev))
        def _():
            self.zin[...] = jnp.zeros_like(self.zin)

    def decays(self, j):
        h = j // SPLIT
        return jnp.exp(self.own_tot[h, 0:1, 0:1]), jnp.exp(self.other_tot[h, 0:1, 0:1])

    def step(self, own):
        s = self.inside
        for j in range(self.count):
            mine, others = self.decays(j)

            @pl.when(self.prev)
            def _():
                self.z_copy(j).wait_recv()

            z = self.zin[j].astype(F32)
            i = own[j]
            self.zout[j] = (mine * others * z + (s * others + (1.0 - s)) * i).astype(BF16)

            @pl.when(self.next)
            def _():
                self.z_copy(j).start()

            self.mout[j] = ((s * mine + (1.0 - s)) * z + s * i).astype(BF16)
            self.m_copy(j).start()

    def result(self, j):
        s = self.inside
        others = self.decays(j)[1]
        self.m_copy(j).wait_recv()
        z = self.zin[j].astype(F32)
        return (self.min[j].astype(F32) + (s + (1.0 - s) * others) * z).astype(BF16)

    def finish(self):
        for j in range(self.count):

            @pl.when(self.next)
            def _():
                self.z_copy(j).wait_send()

            self.m_copy(j).wait_send()


def dot(a, b, da, db):
    return lax.dot_general(a, b, (((da,), (db,)), ((), ())), preferred_element_type=F32)


def flat(block):
    n, cap, q = block.shape
    if cap % 16 == 0:
        return block.reshape(n * cap, q)
    return block.astype(F32).reshape(n * cap, q).astype(BF16)


def swapped(x):
    width = x.shape[1]
    even = lax.rem(lax.broadcasted_iota(jnp.int32, x.shape, 1), 2) == 0
    return jnp.where(even, -pltpu.roll(x, width - 1, 1), pltpu.roll(x, 1, 1))


def whole_kernel(
    n_sp, n_tp, heads,
    stream, og, routes, route_w, queries, keys, values, log_decay, cos_t, sin_t, cos_s, sin_s,
    gate_w, up_w, down_w, proj_w,
    gate_o, up_o, down_o, proj_o, query_o, key_o, value_o,
    full, pack, gu, dw, pw, act, gug, back, part, xbuf, xrecv, sendbuf, ret,
    pick, wcol, slotmap, weight_map, resid, rcols, normed_own, normed_all, normed_f, inv, dec, rem_,
    mask, wts, qr, kr, val, cosb, sinb, totb, toto, inner, inner_g, incoming, proj,
    fzin, fzout, fmin, fmout, bzin, bzout, bmin, bmout,
    wsem, tsem, ssem, rsem, fs, fr, ns, nr, es, er, ps, pr, xs, xr, hs, hr, gs, gr,
    cs, cr, ds, dr, *more,
):
    fsem, bsem, chain_sem = more[0:4], more[4:8], more[8:12]
    me = lax.axis_index("sp")
    c = lax.axis_index("tp")
    core, plane = lax.rem(c, 2), c // 2
    ocore, oplane = 1 - core, 1 - plane
    far = lax.rem(c + n_tp // 2, n_tp)
    near = c + 1 - 2 * core
    other = me + 1 - 2 * lax.rem(me, 2)
    cap, q = full.shape[4:]
    hid = dw.shape[0]
    tokens = stream.shape[0]
    kd = cos_t.shape[1]
    vd = values.shape[2]
    scale = kd ** (-0.5)
    bits = [1 << b for b in range((n_sp - 1).bit_length())]

    def peer(k):
        out = 0
        for b in bits:
            out = out + b * lax.rem(me // b + k // b, 2)
        return out

    loads = [
        pltpu.make_async_copy(gate_w.at[0], gu.at[:, pl.ds(0, hid)], wsem.at[0]),
        pltpu.make_async_copy(up_w.at[0], gu.at[:, pl.ds(hid, hid)], wsem.at[1]),
        pltpu.make_async_copy(down_w.at[0], dw, wsem.at[2]),
        pltpu.make_async_copy(proj_w, pw, wsem.at[3]),
    ]
    for cp in loads:
        cp.start()
    barrier = pltpu.get_barrier_semaphore()

    def hello(k, carry):
        pl.semaphore_signal(barrier, inc=1, device_id=(peer(k), c), device_id_type=MESH)
        return carry

    lax.fori_loop(1, n_sp, hello, 0)
    for t in (far, near):
        pl.semaphore_signal(barrier, inc=1, device_id=(me, t), device_id_type=MESH)

    def cols(index):
        return pl.ds(pl.multiple_of(index * q, 128), q)

    expert = lax.broadcasted_iota(jnp.int32, (n_sp, tokens), 0)
    first_of = expert == routes[0:1, :]
    second_of = expert == routes[1:2, :]
    chosen = first_of | second_of
    weight_map[...] = jnp.where(first_of, route_w[0:1, :], 0.0) + jnp.where(
        second_of, route_w[1:2, :], 0.0
    )
    row = lax.broadcasted_iota(jnp.int32, (tokens, tokens), 0)
    col = lax.broadcasted_iota(jnp.int32, (tokens, tokens), 1)
    earlier = jnp.where(row < col, 1.0, 0.0).astype(BF16)
    before = dot(jnp.where(chosen, 1.0, 0.0).astype(BF16), earlier, 1, 0)
    slotmap[...] = jnp.where(chosen, before, -1.0)
    place = lax.broadcasted_iota(jnp.int32, (cap, tokens), 0).astype(F32)
    for e in range(n_sp):
        hit = jnp.where(slotmap[e : e + 1, :] == place, 1.0, 0.0)
        pick[e] = hit.astype(BF16)
        wcol[e] = jnp.sum(hit * weight_map[e : e + 1, :], axis=1, keepdims=True)

    def fill(spot, e, index):
        rows = dot(pick[e], stream[:, cols(index)], 1, 0)
        grads = wcol[e] * dot(pick[e], og[:, cols(index)], 1, 0)
        spot[0] = rows.astype(BF16)
        spot[1] = grads.astype(BF16)

    half_sp = n_sp // 2

    def turn_of(n):
        return n // 2 + lax.rem(n, 2) * half_sp

    def direct(k, act):
        @pl.when(k < half_sp)
        def _():
            act()

    def crossing(k, act):
        @pl.when(k >= half_sp)
        def _():
            act()

    def out_copy(k):
        return push(
            pack.at[k, plane], full.at[me, core, plane], ssem.at[k], rsem.at[k], (peer(k), c)
        )

    def out_pair(k):
        return push(pack.at[k], full.at[me, core], ssem.at[k], rsem.at[k], (peer(k), c))

    def send_out(k):
        direct(k, lambda: out_pair(k).start())
        crossing(k, lambda: out_copy(k).start())

    def fill_out(k):
        fill(pack.at[k, plane], peer(k), c)
        direct(k, lambda: fill(pack.at[k, oplane], peer(k), far))

    def far_copy(k, p):
        spot = full.at[peer(k), core, p]
        return push(spot, spot, fs.at[k], fr.at[k], (me, far))

    def near_copy(k, side):
        spot = full.at[peer(k), side, plane]
        return push(spot, spot, ns.at[k], nr.at[k], (me, near))

    def near_pair(k, side):
        spot = full.at[peer(k), side]
        return push(spot, spot, ns.at[k], nr.at[k], (me, near))

    def relay_copy(k, side):
        spot = full.at[peer(k), side, oplane]
        return push(spot, spot, es.at[k], er.at[k], (me, near))

    def part_copy(k):
        return push(back.at[k, ocore], part.at[k], ps.at[k], pr.at[k], (me, near))

    def x_copy(k):
        return push(xbuf.at[k], xrecv.at[k], xs.at[k], xr.at[k], (me, far))

    def home_copy(k):
        return push(sendbuf.at[k], ret.at[k], hs.at[k], hr.at[k], (peer(k), c))

    fill(pack.at[half_sp, plane], peer(half_sp), c)
    fill_out(1)
    running = lax.dot_general(
        log_decay[...], jnp.where(row <= col, 1.0, 0.0), (((1,), (0,)), ((), ())),
        preferred_element_type=F32, precision=lax.Precision.HIGHEST,
    )
    for h in range(heads):
        totb[h] = jnp.broadcast_to(running[h : h + 1, tokens - 1 : tokens], totb.shape[1:])
    start_cos, start_sin = cos_s[pl.ds(me, 1), :], sin_s[pl.ds(me, 1), :]
    cosines = start_cos * cos_t[...] - start_sin * sin_t[...]
    sines = start_sin * cos_t[...] + start_cos * sin_t[...]
    cosb[...] = cosines
    sinb[...] = sines
    rows_of = kd // SPLIT
    for h in range(heads):
        x = queries[:, h, :].astype(F32)
        qr[h] = (x * cosines + swapped(x) * sines).astype(BF16)
        x = keys[:, h, :].astype(F32)
        key = (x * cosines + swapped(x) * sines) * scale
        kr[h] = key.astype(BF16)
        val[h] = values[:, h, :]
        along = jnp.broadcast_to(running[h : h + 1, :], (tokens, tokens))
        down = along.T
        run = down[:, 0:1]
        left = jnp.exp(running[h : h + 1, tokens - 1 : tokens] - run)
        dec[h] = jnp.exp(run)
        rem_[h] = left
        state = dot((key * left).astype(BF16), val[h], 0, 0)
        for s in range(SPLIT):
            inner[h * SPLIT + s] = state[s * rows_of : (s + 1) * rows_of]
        causal = row >= col
        mask[h] = jnp.where(causal, jnp.exp(jnp.where(causal, down - along, 0.0)), 0.0)
    totals = (totb, toto)
    past = Scan(True, n_sp, me, c, (fzin, fzout, fmin, fmout), fsem, totals, heads)
    coming = Scan(False, n_sp, me, c, (bzin, bzout, bmin, bmout), bsem, totals, heads)
    past.clear()
    coming.clear()
    pairs = n_sp // 2
    pace = (n_sp + 4) // pairs
    early = n_sp * 3 // 4
    pl.semaphore_wait(barrier, n_sp - 1 + 2)
    swap_tot = push(totb, toto, tsem.at[0], tsem.at[1], (other, c))
    swap_tot.start()
    out_copy(half_sp).start()
    out_pair(1).start()
    fill(full.at[me, core, plane], me, c)
    fill(full.at[me, core, oplane], me, far)
    near_pair(0, core).start()

    def fill_rest(n, carry):
        fill_out(turn_of(n))
        return carry

    def send_rest(n, carry):
        send_out(turn_of(n))
        return carry

    lax.fori_loop(3, n_sp, fill_rest, 0)
    swap_tot.wait()

    @pl.when(past.slot == 0)
    def _():
        past.step(inner)

    lax.fori_loop(3, early, send_rest, 0)
    for cp in loads:
        cp.wait()

    def compute(k):
        src = peer(k)

        @pl.when(k < half_sp)
        def _():
            near_pair(k, ocore).wait_recv()

        @pl.when(k >= half_sp)
        def _():
            near_copy(k, ocore).wait_recv()
            relay_copy(k, ocore).wait_recv()

        pre = 0.0
        act_grad = 0.0
        for t in range(n_tp):
            band = pl.ds(t * q, q)
            spot = full.at[src, t % 2, t // 2]
            pre = pre + dot(spot[0], gu[band, :], 1, 0)
            act_grad = act_grad + dot(spot[1], dw[:, band], 1, 1)
        gate_pre = pre[:, :hid]
        up_pre = pre[:, hid:]
        gate_clip = jnp.minimum(gate_pre, CLAMP_LIMIT)
        up_clip = jnp.clip(up_pre, -CLAMP_LIMIT, CLAMP_LIMIT)
        sig = 1.0 / (1.0 + jnp.exp(-GATE_SLOPE * gate_clip))
        gated = gate_clip * sig
        act[src] = (gated * (up_clip + 1.0)).astype(BF16)
        slope = sig + GATE_SLOPE * gated * (1.0 - sig)
        gpg = jnp.where(gate_pre < CLAMP_LIMIT, act_grad * (up_clip + 1.0) * slope, 0.0)
        upg = jnp.where(jnp.abs(up_pre) < CLAMP_LIMIT, act_grad * gated, 0.0)
        both = jnp.concatenate([gpg, upg], axis=1).astype(BF16)
        gug[src] = both
        for t in range(n_tp):
            back[k, t % 2, t // 2] = dot(both, gu[pl.ds(t * q, q), :], 1, 1).astype(BF16)
        part_copy(k).start()

    def first(k):
        part_copy(k).wait_recv()
        xbuf[k] = (back[k, core, oplane].astype(F32) + part[k, oplane].astype(F32)).astype(BF16)
        x_copy(k).start()

    def second(k):
        x_copy(k).wait_recv()
        total = (
            back[k, core, plane].astype(F32) + part[k, plane].astype(F32) + xrecv[k].astype(F32)
        ).astype(BF16)

        @pl.when(k == 0)
        def _():
            ret[0] = total

        @pl.when(k > 0)
        def _():
            sendbuf[k] = total
            home_copy(k).start()

    def local_retention():
        for h in range(heads):
            score = dot(qr[h], kr[h], 1, 1) * mask[h]
            wts[h] = score.astype(BF16)
            normed_f[:, h * vd : (h + 1) * vd] = dot(wts[h], val[h], 1, 0)

    compute(0)
    local_retention()

    def step(n, carry):
        k = turn_of(n)

        @pl.when((n < n_sp) & (k < half_sp))
        def _():
            spot = full.at[peer(k), core]
            push(spot, spot, ssem.at[k], rsem.at[k], (me, far)).wait_recv()
            near_pair(k, core).start()

        @pl.when((n < n_sp) & (k >= half_sp))
        def _():
            spot = full.at[peer(k), core, plane]
            push(spot, spot, ssem.at[k], rsem.at[k], (me, far)).wait_recv()
            far_copy(k, plane).start()
            near_copy(k, core).start()

        j = turn_of(n - 1)

        @pl.when((n <= n_sp) & (j >= half_sp))
        def _():
            far_copy(j, oplane).wait_recv()
            relay_copy(j, core).start()

        @pl.when((n == past.slot * pace) & (past.slot > 0))
        def _():
            past.step(inner)

        @pl.when(n == pace)
        def _():
            lax.fori_loop(early, n_sp, send_rest, 0)

        @pl.when(n == 1)
        def _():
            first(0)

        @pl.when(n == 2)
        def _():
            second(0)

        @pl.when((n >= 3) & (n < n_sp + 2))
        def _():
            compute(turn_of(n - 2))

        @pl.when((n >= 4) & (n < n_sp + 3))
        def _():
            first(turn_of(n - 3))

        @pl.when((n >= 5) & (n < n_sp + 4))
        def _():
            second(turn_of(n - 4))

        return carry

    lax.fori_loop(1, n_sp + 4, step, 0)

    for j in range(heads * SPLIT):
        incoming[j // SPLIT, pl.ds((j % SPLIT) * rows_of, rows_of), :] = past.result(j)
    for h in range(heads):
        band = slice(h * vd, (h + 1) * vd)
        kept = normed_f[:, band] + dec[h] * dot(qr[h], incoming[h], 1, 0)
        inverse = lax.rsqrt(jnp.mean(kept * kept, axis=1, keepdims=True) + EPSILON)
        inv[h] = inverse
        normed_f[:, band] = kept * inverse
        normed_own[:, band] = (kept * inverse).astype(BF16)
    normed_all[me] = normed_own[...]
    spread = Chain(normed_own, normed_all, n_sp, me, c, chain_sem, (0, 1))
    spread.start()

    def arrive(k, total):
        push(sendbuf.at[k], ret.at[k], hs.at[k], hr.at[k], (me, far)).wait_recv()
        return total + dot(pick[peer(k)], ret[k], 0, 0)

    total = og[:, cols(c)].astype(F32) + dot(pick[me], ret[0], 0, 0)
    total = lax.fori_loop(1, n_sp, arrive, total)
    half = tokens // 2
    resid[core, plane] = total.astype(BF16)

    def strip(side, p, i):
        return resid.at[side, p, pl.ds(i * half, half)]

    sent = []
    for i in range(2):
        mine = strip(core, plane, i)
        sent.append(push(mine, mine, gs.at[0, i], gr.at[0, i], (me, far)))
    for i in range(2):
        mine = strip(core, plane, i)
        sent.append(push(mine, mine, gs.at[1, i], gr.at[1, i], (me, near)))
    for cp in sent:
        cp.start()
    spread.step(1)

    def share(side, p):
        return dot(resid[side, p], pw[cols(2 * p + side), :], 1, 0)

    normed_grad = share(core, plane)
    for i in range(2):
        spot = strip(core, oplane, i)
        push(spot, spot, gs.at[0, i], gr.at[0, i], (me, far)).wait_recv()
        onward = push(spot, spot, gs.at[2, i], gr.at[2, i], (me, near))
        onward.start()
        sent.append(onward)
    normed_grad = normed_grad + share(core, oplane)
    for j, p in ((1, plane), (2, oplane)):
        for i in range(2):
            spot = strip(ocore, p, i)
            push(spot, spot, gs.at[j, i], gr.at[j, i], (me, near)).wait_recv()
        normed_grad = normed_grad + share(ocore, p)

    group = rcols.shape[3]
    per_quarter = q // group
    per_group = group * n_sp // (q * n_tp)

    def band_of(index):
        g = index // per_group
        quarter = g // per_quarter
        return resid.at[
            lax.rem(quarter, 2), quarter // 2, pl.ds(core * half, half),
            pl.ds(pl.multiple_of(lax.rem(g, per_quarter) * group, 128), group),
        ]

    def col_copy(k):
        return push(band_of(peer(k)), rcols.at[me, core], cs.at[k], cr.at[k], (peer(k), c))

    def col_near(k, side):
        spot = rcols.at[peer(k), side]
        return push(spot, spot, ds.at[k], dr.at[k], (me, near))

    def send_cols(k, carry):
        col_copy(k).start()
        return carry

    grads = []
    for h in range(heads):
        band = slice(h * vd, (h + 1) * vd)
        ng = normed_grad[:, band]
        nf = normed_f[:, band]
        grad = inv[h] * (ng - nf * jnp.mean(ng * nf, axis=1, keepdims=True))
        grad_bf = grad.astype(BF16)
        grads.append(grad_bf)
        turned = (qr[h].astype(F32) * dec[h]).astype(BF16)
        state = dot(turned, grad_bf, 0, 0)
        for s in range(SPLIT):
            inner_g[h * SPLIT + s] = state[s * rows_of : (s + 1) * rows_of]

    def weights_grad(t):
        x = flat(full[:, lax.rem(t, 2), t // 2, 0])
        g = flat(full[:, lax.rem(t, 2), t // 2, 1])
        both = dot(x, flat(gug[...]), 0, 0).astype(BF16)
        gate_o[0, cols(t), :] = both[:, :hid]
        up_o[0, cols(t), :] = both[:, hid:]
        down_o[0, :, cols(t)] = dot(flat(act[...]), g, 0, 0).astype(BF16)

    @pl.when(coming.slot == 0)
    def _():
        coming.step(inner_g)

    lax.fori_loop(1, n_sp, send_cols, 0)

    def late(s, carry):
        @pl.when((s == coming.slot) & (s > 0))
        def _():
            coming.step(inner_g)

        if pairs > 2:

            @pl.when(s == 1)
            def _():
                spread.step(2)

        @pl.when(s < n_tp)
        def _():
            weights_grad(s)

        return carry

    lax.fori_loop(0, max(pairs, n_tp), late, 0)
    for d in range(3, pairs):
        spread.step(d)
    for side in range(2):
        g = me // per_group
        quarter = g // per_quarter
        rcols[me, side] = resid[
            lax.rem(quarter, 2), quarter // 2, side * half : (side + 1) * half,
            pl.ds(pl.multiple_of(lax.rem(g, per_quarter) * group, 128), group),
        ]

    def relay_cols(k, carry):
        spot = rcols.at[peer(k), core]
        push(spot, spot, cs.at[k], cr.at[k], (me, far)).wait_recv()
        col_near(k, core).start()
        return carry

    lax.fori_loop(1, n_sp, relay_cols, 0)

    def unturn(x):
        return x * cosb[...] - swapped(x) * sinb[...]

    partial = []
    for h in range(heads):
        score = (dot(grads[h], val[h], 1, 1) * mask[h]).astype(BF16)
        qp = dot(score, kr[h], 1, 0) + dec[h] * dot(grads[h], incoming[h], 1, 1)
        query_o[:, h * kd : (h + 1) * kd] = unturn(qp).astype(BF16)
        partial.append((dot(score, qr[h], 0, 0), dot(wts[h], grads[h], 0, 0)))

    def near_cols(k, carry):
        col_near(k, ocore).wait_recv()
        return carry

    lax.fori_loop(1, n_sp, near_cols, 0)
    spread.finish()
    columns = rcols[...].reshape(n_sp * tokens, group)
    everyone = normed_all[...].reshape(n_sp * tokens, heads * vd)
    proj[...] = dot(columns, everyone, 0, 0)
    width = proj_o.shape[0]
    proj_o[...] = proj[pl.ds(pl.multiple_of(lax.rem(me, per_group) * width, 8), width), :]

    future = [coming.result(j) for j in range(heads * SPLIT)]
    for h in range(heads):
        band = slice(h * vd, (h + 1) * vd)
        key_part, value_part = partial[h]
        later = jnp.concatenate(future[h * SPLIT : (h + 1) * SPLIT], axis=0)
        kp = key_part + rem_[h] * dot(val[h], later, 1, 1)
        key_o[:, h * kd : (h + 1) * kd] = (unturn(kp) * scale).astype(BF16)
        value_o[:, band] = (value_part + rem_[h] * dot(kr[h], later, 1, 0)).astype(BF16)

    for cp in sent:
        cp.wait_send()
    past.finish()
    coming.finish()

    def drain(k, carry):
        part_copy(k).wait_send()
        x_copy(k).wait_send()

        @pl.when(k < half_sp)
        def _():
            near_pair(k, core).wait_send()

        @pl.when((k > 0) & (k < half_sp))
        def _():
            out_pair(k).wait_send()

        @pl.when(k >= half_sp)
        def _():
            out_copy(k).wait_send()
            far_copy(k, plane).wait_send()
            near_copy(k, core).wait_send()
            relay_copy(k, core).wait_send()

        @pl.when(k > 0)
        def _():
            home_copy(k).wait_send()
            col_copy(k).wait_send()
            col_near(k, core).wait_send()

        return carry

    lax.fori_loop(0, n_sp, drain, 0)


def finish_kernel(
    gate, up, down, proj, query, key, value, gate_o, up_o, down_o, proj_o, query_o, key_o, value_o,
    sem,
):
    pairs = ((gate, gate_o), (up, up_o), (down, down_o), (proj, proj_o))
    stores = [pltpu.make_async_copy(a, b, sem.at[i]) for i, (a, b) in enumerate(pairs)]
    for cp in stores:
        cp.start()
    for a, b in ((query, query_o), (key, key_o), (value, value_o)):
        width = b.shape[2]
        for h in range(b.shape[1]):
            b[:, h, :] = a[:, h * width : (h + 1) * width]
    for cp in stores:
        cp.wait()


def rotation_tables(n_sp, tokens, key_width):
    frequency = 10000.0 ** -np.linspace(0.0, 1.0, key_width // 2)
    frequency = np.repeat(frequency, 2)
    angle = np.arange(tokens)[:, None] * frequency[None, :]
    start = tokens * np.arange(n_sp)[:, None] * frequency[None, :]
    return [
        jnp.asarray(table.astype(np.float32))
        for table in (np.cos(angle), np.sin(angle), np.cos(start), np.sin(start))
    ]


def per_device(
    stream, out_grad, routes, route_weight, queries, key_vectors, value_vectors, log_decay,
    out_proj, gate_weight, up_weight, down_weight,
):
    n_sp = lax.axis_size("sp")
    n_tp = lax.axis_size("tp")
    tokens, width = stream.shape
    cap = 4 * tokens // n_sp
    q = width // n_tp
    heads, kd = queries.shape[1:]
    vd = value_vectors.shape[2]
    hid = gate_weight.shape[2]
    w = width // n_sp
    group = max(w, 128)
    count, rows_of = heads * SPLIT, kd // SPLIT
    vmem, dma = pltpu.VMEM, pltpu.SemaphoreType.DMA
    block = vmem((n_sp, cap, q), BF16)
    packet = vmem((count, rows_of, vd), BF16)
    tables = rotation_tables(n_sp, tokens, kd)
    outs = pl.pallas_call(
        functools.partial(whole_kernel, n_sp, n_tp, heads),
        out_shape=(
            vmem(gate_weight.shape, BF16),
            vmem(up_weight.shape, BF16),
            vmem(down_weight.shape, BF16),
            vmem((w, heads * vd), F32),
            vmem((tokens, heads * kd), BF16),
            vmem((tokens, heads * kd), BF16),
            vmem((tokens, heads * vd), BF16),
        ),
        in_specs=vmem_specs(12) + [pl.BlockSpec(memory_space=pltpu.HBM)] * 4,
        out_specs=tuple(vmem_specs(7)),
        scratch_shapes=[
            vmem((n_sp, 2, 2, 2, cap, q), BF16),
            vmem((n_sp, 2, 2, cap, q), BF16),
            vmem((width, 2 * hid), BF16),
            vmem((hid, width), BF16),
            vmem((width, heads * vd), BF16),
            vmem((n_sp, cap, hid), BF16),
            vmem((n_sp, cap, 2 * hid), BF16),
            vmem((n_sp, 2, 2, cap, q), BF16),
            vmem((n_sp, 2, cap, q), BF16),
            block, block, block, block,
            vmem((n_sp, cap, tokens), BF16),
            vmem((n_sp, cap, 1), F32),
            vmem((n_sp, tokens), F32),
            vmem((n_sp, tokens), F32),
            vmem((2, 2, tokens, q), BF16),
            vmem((n_sp, 2, tokens // 2, group), BF16),
            vmem((tokens, heads * vd), BF16),
            vmem((n_sp, tokens, heads * vd), BF16),
            vmem((tokens, heads * vd), F32),
            vmem((heads, tokens, 1), F32),
            vmem((heads, tokens, 1), F32),
            vmem((heads, tokens, 1), F32),
            vmem((heads, tokens, tokens), F32),
            vmem((heads, tokens, tokens), BF16),
            vmem((heads, tokens, kd), BF16),
            vmem((heads, tokens, kd), BF16),
            vmem((heads, tokens, vd), BF16),
            vmem((tokens, kd), F32),
            vmem((tokens, kd), F32),
            vmem((heads, 8, 128), F32),
            vmem((heads, 8, 128), F32),
            vmem((count, rows_of, vd), F32),
            vmem((count, rows_of, vd), F32),
            vmem((heads, kd, vd), BF16),
            vmem((group, heads * vd), F32),
        ]
        + [packet] * 8
        + [dma((4,)), dma((2,))]
        + [dma((n_sp,))] * 14
        + [dma((3, 2))] * 2
        + [dma((n_sp,))] * 4
        + [dma((count,))] * 8
        + [dma((2, n_sp // 2))] * 4,
        compiler_params=pltpu.CompilerParams(
            collective_id=0, has_side_effects=True, vmem_limit_bytes=58 * 2**20
        ),
        name="whole",
    )(
        stream, out_grad, routes.T, route_weight.T, queries, key_vectors, value_vectors,
        log_decay.T, *tables, gate_weight, up_weight, down_weight, out_proj,
    )
    shapes = [jax.ShapeDtypeStruct(x.shape, x.dtype) for x in outs[:4]] + [
        jax.ShapeDtypeStruct(x.shape, BF16) for x in (queries, key_vectors, value_vectors)
    ]
    return pl.pallas_call(
        finish_kernel,
        out_shape=tuple(shapes),
        in_specs=vmem_specs(7),
        out_specs=tuple(any_specs(4) + vmem_specs(3)),
        scratch_shapes=[dma((4,))],
        compiler_params=pltpu.CompilerParams(vmem_limit_bytes=16 * 2**20),
        name="finish",
    )(*outs)


def solution(mesh):
    in_specs = (
        P("sp", None),
        P("sp", None),
        P("sp", None),
        P("sp", None),
        P("sp", "tp", None),
        P("sp", "tp", None),
        P("sp", "tp", None),
        P("sp", "tp"),
        P(None, "tp"),
        P("sp", None, "tp"),
        P("sp", None, "tp"),
        P("sp", "tp", None),
    )
    out_specs = (
        P("sp", None, "tp"),
        P("sp", None, "tp"),
        P("sp", "tp", None),
        P("sp", "tp"),
        P("sp", "tp", None),
        P("sp", "tp", None),
        P("sp", "tp", None),
    )
    return jax.shard_map(
        per_device, mesh=mesh, in_specs=in_specs, out_specs=out_specs, check_vma=False
    )
```

```python
import functools

import jax
import jax.numpy as jnp
import numpy as np
from jax import lax
from jax.experimental import pallas as pl
from jax.experimental.pallas import tpu as pltpu
from jax.sharding import PartitionSpec as P

CLAMP_LIMIT = 7.0
GATE_SLOPE = 1.702
EPSILON = 1e-06
F32 = jnp.float32
BF16 = jnp.bfloat16
MESH = pl.DeviceIdType.MESH
SPLIT = 2


def any_specs(count):
    return [pl.BlockSpec(memory_space=pl.ANY)] * count


def vmem_specs(count):
    return [pl.BlockSpec(memory_space=pltpu.VMEM)] * count


def push(src, dst, send_sem, recv_sem, device):
    return pltpu.make_async_remote_copy(
        src_ref=src,
        dst_ref=dst,
        send_sem=send_sem,
        recv_sem=recv_sem,
        device_id=device,
        device_id_type=MESH,
    )


class Chain:
    def __init__(self, src, out, n_sp, me, c, sems, ways):
        self.src, self.out, self.me, self.c = src, out, me, c
        self.pairs, self.ways = n_sp // 2, ways
        self.pair = me // 2
        self.other = me + 1 - 2 * lax.rem(me, 2)
        self.zs, self.zr, self.ys, self.yr = sems

    def has(self, d, way):
        return self.pair >= d if way == 0 else self.pair + d < self.pairs

    def room(self, way):
        return self.pair + 1 < self.pairs if way == 0 else self.pair >= 1

    def spot(self, base, d, way):
        return self.out.at[base - 2 * d if way == 0 else base + 2 * d]

    def along(self, d, way):
        spot = self.spot(self.me, d, way)
        return push(
            self.src if d == 0 else spot, spot, self.zs.at[way, d], self.zr.at[way, d + 1],
            (self.me + 2 if way == 0 else self.me - 2, self.c),
        )

    def across(self, d, way):
        spot = self.spot(self.me, d, way)
        return push(
            self.src if d == 0 else spot, spot, self.ys.at[way, d], self.yr.at[way, d],
            (self.other, self.c),
        )

    def each(self, d, act):
        for way in self.ways:

            @pl.when(self.has(d, way))
            def _():
                if d < self.pairs - 1:

                    @pl.when(self.room(way))
                    def _():
                        act(self.along(d, way))

                if d > 0 or way == self.ways[0]:
                    act(self.across(d, way))

    def start(self):
        self.each(0, lambda cp: cp.start())

    def step(self, d):
        for way in self.ways:

            @pl.when(self.has(d, way))
            def _():
                spot = self.spot(self.me, d, way)
                push(
                    spot, spot, self.zs.at[way, d], self.zr.at[way, d], (self.other, self.c)
                ).wait_recv()

        self.each(d, lambda cp: cp.start())

    def finish(self):
        for d in range(self.pairs):
            for way in self.ways:
                if d == 0 and way != self.ways[0]:
                    continue

                @pl.when(self.has(d, way))
                def _():
                    spot = self.spot(self.other, d, way)
                    push(
                        spot, spot, self.ys.at[way, d], self.yr.at[way, d], (self.other, self.c)
                    ).wait_recv()

            self.each(d, lambda cp: cp.wait_send())


class Scan:
    def __init__(self, forward, n_sp, me, c, bufs, sems, totals, heads):
        self.forward, self.me, self.c = forward, me, c
        self.zin, self.zout, self.min, self.mout = bufs
        self.zs, self.zr, self.ms, self.mr = sems
        self.own_tot, self.other_tot = totals
        pairs = n_sp // 2
        pair = me // 2
        parity = lax.rem(me, 2)
        self.other = me + 1 - 2 * parity
        self.prev = pair > 0 if forward else pair + 1 < pairs
        self.next = pair + 1 < pairs if forward else pair > 0
        self.ahead = me + 2 if forward else me - 2
        self.slot = pair if forward else pairs - 1 - pair
        self.inside = jnp.where(parity == (0 if forward else 1), 1.0, 0.0)
        self.count = heads * SPLIT

    def z_copy(self, j):
        return push(
            self.zout.at[j], self.zin.at[j], self.zs.at[j], self.zr.at[j], (self.ahead, self.c)
        )

    def m_copy(self, j):
        return push(
            self.mout.at[j], self.min.at[j], self.ms.at[j], self.mr.at[j], (self.other, self.c)
        )

    def clear(self):
        @pl.when(jnp.logical_not(self.prev))
        def _():
            self.zin[...] = jnp.zeros_like(self.zin)

    def decays(self, j):
        h = j // SPLIT
        return jnp.exp(self.own_tot[h, 0:1, 0:1]), jnp.exp(self.other_tot[h, 0:1, 0:1])

    def step(self, own):
        s = self.inside
        for j in range(self.count):
            mine, others = self.decays(j)

            @pl.when(self.prev)
            def _():
                self.z_copy(j).wait_recv()

            z = self.zin[j].astype(F32)
            i = own[j]
            self.zout[j] = (mine * others * z + (s * others + (1.0 - s)) * i).astype(BF16)

            @pl.when(self.next)
            def _():
                self.z_copy(j).start()

            self.mout[j] = ((s * mine + (1.0 - s)) * z + s * i).astype(BF16)
            self.m_copy(j).start()

    def result(self, j):
        s = self.inside
        others = self.decays(j)[1]
        self.m_copy(j).wait_recv()
        z = self.zin[j].astype(F32)
        return (self.min[j].astype(F32) + (s + (1.0 - s) * others) * z).astype(BF16)

    def finish(self):
        for j in range(self.count):

            @pl.when(self.next)
            def _():
                self.z_copy(j).wait_send()

            self.m_copy(j).wait_send()


def dot(a, b, da, db):
    return lax.dot_general(a, b, (((da,), (db,)), ((), ())), preferred_element_type=F32)


def fine(a, b, da, db):
    return lax.dot_general(
        a.astype(F32), b.astype(F32), (((da,), (db,)), ((), ())), preferred_element_type=F32,
        precision=lax.Precision.HIGHEST,
    )


def flat(block):
    n, cap, q = block.shape
    if cap % 16 == 0:
        return block.reshape(n * cap, q)
    return block.astype(F32).reshape(n * cap, q).astype(BF16)


def swapped(x):
    width = x.shape[1]
    even = lax.rem(lax.broadcasted_iota(jnp.int32, x.shape, 1), 2) == 0
    return jnp.where(even, -pltpu.roll(x, width - 1, 1), pltpu.roll(x, 1, 1))


def whole_kernel(
    n_sp, n_tp, heads,
    stream, og, routes, route_w, queries, keys, values, log_decay, cos_t, sin_t, cos_s, sin_s,
    gate_w, up_w, down_w, proj_w,
    gate_o, up_o, down_o, proj_o, query_o, key_o, value_o,
    full, pack, gu, dw, pw, act, gug, back, part, xbuf, xrecv, sendbuf, ret,
    pick, wcol, slotmap, weight_map, resid, rcols, normed_own, normed_all, normed_f, inv, dec, rem_,
    mask, wts, qr, kr, qrf, krf, grad_f, val, cosb, sinb, totb, toto, inner, inner_g, incoming, proj,
    fzin, fzout, fmin, fmout, bzin, bzout, bmin, bmout,
    wsem, tsem, ssem, rsem, fs, fr, ns, nr, es, er, ps, pr, xs, xr, hs, hr, gs, gr,
    cs, cr, ds, dr, as_, ar, bs, br, *more,
):
    fsem, bsem, chain_sem = more[0:4], more[4:8], more[8:12]
    me = lax.axis_index("sp")
    c = lax.axis_index("tp")
    core, plane = lax.rem(c, 2), c // 2
    ocore, oplane = 1 - core, 1 - plane
    far = lax.rem(c + n_tp // 2, n_tp)
    near = c + 1 - 2 * core
    near_far = lax.rem(near + n_tp // 2, n_tp)
    other = me + 1 - 2 * lax.rem(me, 2)
    cap, q = full.shape[4:]
    hid = dw.shape[0]
    tokens = stream.shape[0]
    kd = cos_t.shape[1]
    vd = values.shape[2]
    scale = kd ** (-0.5)
    bits = [1 << b for b in range((n_sp - 1).bit_length())]

    def peer(k):
        out = 0
        for b in bits:
            out = out + b * lax.rem(me // b + k // b, 2)
        return out

    loads = [
        pltpu.make_async_copy(gate_w.at[0], gu.at[:, pl.ds(0, hid)], wsem.at[0]),
        pltpu.make_async_copy(up_w.at[0], gu.at[:, pl.ds(hid, hid)], wsem.at[1]),
        pltpu.make_async_copy(down_w.at[0], dw, wsem.at[2]),
        pltpu.make_async_copy(proj_w, pw, wsem.at[3]),
    ]
    for cp in loads:
        cp.start()
    barrier = pltpu.get_barrier_semaphore()

    def hello(k, carry):
        pl.semaphore_signal(barrier, inc=1, device_id=(peer(k), c), device_id_type=MESH)
        return carry

    lax.fori_loop(1, n_sp, hello, 0)
    for t in (far, near):
        pl.semaphore_signal(barrier, inc=1, device_id=(me, t), device_id_type=MESH)

    def cols(index):
        return pl.ds(pl.multiple_of(index * q, 128), q)

    expert = lax.broadcasted_iota(jnp.int32, (n_sp, tokens), 0)
    first_of = expert == routes[0:1, :]
    second_of = expert == routes[1:2, :]
    chosen = first_of | second_of
    weight_map[...] = jnp.where(first_of, route_w[0:1, :], 0.0) + jnp.where(
        second_of, route_w[1:2, :], 0.0
    )
    row = lax.broadcasted_iota(jnp.int32, (tokens, tokens), 0)
    col = lax.broadcasted_iota(jnp.int32, (tokens, tokens), 1)
    earlier = jnp.where(row < col, 1.0, 0.0).astype(BF16)
    before = dot(jnp.where(chosen, 1.0, 0.0).astype(BF16), earlier, 1, 0)
    slotmap[...] = jnp.where(chosen, before, -1.0)
    place = lax.broadcasted_iota(jnp.int32, (cap, tokens), 0).astype(F32)
    for e in range(n_sp):
        hit = jnp.where(slotmap[e : e + 1, :] == place, 1.0, 0.0)
        pick[e] = hit.astype(BF16)
        wcol[e] = jnp.sum(hit * weight_map[e : e + 1, :], axis=1, keepdims=True)

    def fill(spot, e, index):
        rows = dot(pick[e], stream[:, cols(index)], 1, 0)
        grads = wcol[e] * dot(pick[e], og[:, cols(index)], 1, 0)
        spot[0] = rows.astype(BF16)
        spot[1] = grads.astype(BF16)

    half_sp = n_sp // 2

    def turn_of(n):
        return n // 2 + lax.rem(n, 2) * half_sp

    def direct(k, act):
        @pl.when(k < half_sp)
        def _():
            act()

    def crossing(k, act):
        @pl.when(k >= half_sp)
        def _():
            act()

    def out_copy(k):
        return push(
            pack.at[k, plane], full.at[me, core, plane], ssem.at[k], rsem.at[k], (peer(k), c)
        )

    def out_pair(k):
        return push(pack.at[k], full.at[me, core], ssem.at[k], rsem.at[k], (peer(k), c))

    def send_out(k):
        direct(k, lambda: out_pair(k).start())
        crossing(k, lambda: out_copy(k).start())

    def fill_out(k):
        fill(pack.at[k, plane], peer(k), c)
        direct(k, lambda: fill(pack.at[k, oplane], peer(k), far))

    def far_copy(k, p):
        spot = full.at[peer(k), core, p]
        return push(spot, spot, fs.at[k], fr.at[k], (me, far))

    def near_copy(k, side):
        spot = full.at[peer(k), side, plane]
        return push(spot, spot, ns.at[k], nr.at[k], (me, near))

    def near_pair(k, side):
        spot = full.at[peer(k), side]
        return push(spot, spot, ns.at[k], nr.at[k], (me, near))

    def relay_copy(k, side):
        spot = full.at[peer(k), side, oplane]
        return push(spot, spot, es.at[k], er.at[k], (me, near))

    def part_copy(k):
        return push(back.at[k, ocore], part.at[k], ps.at[k], pr.at[k], (me, near))

    def x_copy(k):
        return push(xbuf.at[k], xrecv.at[k], xs.at[k], xr.at[k], (me, far))

    def home_copy(k):
        return push(sendbuf.at[k], ret.at[k], hs.at[k], hr.at[k], (peer(k), c))

    fill(pack.at[half_sp, plane], peer(half_sp), c)
    fill_out(1)
    running = lax.dot_general(
        log_decay[...], jnp.where(row <= col, 1.0, 0.0), (((1,), (0,)), ((), ())),
        preferred_element_type=F32, precision=lax.Precision.HIGHEST,
    )
    for h in range(heads):
        totb[h] = jnp.broadcast_to(running[h : h + 1, tokens - 1 : tokens], totb.shape[1:])
    start_cos, start_sin = cos_s[pl.ds(me, 1), :], sin_s[pl.ds(me, 1), :]
    cosines = start_cos * cos_t[...] - start_sin * sin_t[...]
    sines = start_sin * cos_t[...] + start_cos * sin_t[...]
    cosb[...] = cosines
    sinb[...] = sines
    rows_of = kd // SPLIT
    for h in range(heads):
        x = queries[:, h, :].astype(F32)
        qrf[h] = x * cosines + swapped(x) * sines
        qr[h] = qrf[h].astype(BF16)
        x = keys[:, h, :].astype(F32)
        key = (x * cosines + swapped(x) * sines) * scale
        krf[h] = key
        kr[h] = key.astype(BF16)
        val[h] = values[:, h, :]
        along = jnp.broadcast_to(running[h : h + 1, :], (tokens, tokens))
        down = along.T
        run = down[:, 0:1]
        left = jnp.exp(running[h : h + 1, tokens - 1 : tokens] - run)
        dec[h] = jnp.exp(run)
        rem_[h] = left
        state = dot((key * left).astype(BF16), val[h], 0, 0)
        for s in range(SPLIT):
            inner[h * SPLIT + s] = state[s * rows_of : (s + 1) * rows_of]
        causal = row >= col
        mask[h] = jnp.where(causal, jnp.exp(jnp.where(causal, down - along, 0.0)), 0.0)
    totals = (totb, toto)
    past = Scan(True, n_sp, me, c, (fzin, fzout, fmin, fmout), fsem, totals, heads)
    coming = Scan(False, n_sp, me, c, (bzin, bzout, bmin, bmout), bsem, totals, heads)
    past.clear()
    coming.clear()
    pairs = n_sp // 2
    pace = (n_sp + 4) // pairs
    early = n_sp * 3 // 4
    pl.semaphore_wait(barrier, n_sp - 1 + 2)
    swap_tot = push(totb, toto, tsem.at[0], tsem.at[1], (other, c))
    swap_tot.start()
    out_copy(half_sp).start()
    out_pair(1).start()
    fill(full.at[me, core, plane], me, c)
    fill(full.at[me, core, oplane], me, far)
    near_pair(0, core).start()

    def fill_rest(n, carry):
        fill_out(turn_of(n))
        return carry

    def send_rest(n, carry):
        send_out(turn_of(n))
        return carry

    lax.fori_loop(3, n_sp, fill_rest, 0)
    swap_tot.wait()

    @pl.when(past.slot == 0)
    def _():
        past.step(inner)

    lax.fori_loop(3, early, send_rest, 0)
    for cp in loads:
        cp.wait()

    def compute(k):
        src = peer(k)

        @pl.when(k < half_sp)
        def _():
            near_pair(k, ocore).wait_recv()

        @pl.when(k >= half_sp)
        def _():
            near_copy(k, ocore).wait_recv()
            relay_copy(k, ocore).wait_recv()

        pre = 0.0
        act_grad = 0.0
        for t in range(n_tp):
            band = pl.ds(t * q, q)
            spot = full.at[src, t % 2, t // 2]
            pre = pre + dot(spot[0], gu[band, :], 1, 0)
            act_grad = act_grad + dot(spot[1], dw[:, band], 1, 1)
        gate_pre = pre[:, :hid]
        up_pre = pre[:, hid:]
        gate_clip = jnp.minimum(gate_pre, CLAMP_LIMIT)
        up_clip = jnp.clip(up_pre, -CLAMP_LIMIT, CLAMP_LIMIT)
        sig = 1.0 / (1.0 + jnp.exp(-GATE_SLOPE * gate_clip))
        gated = gate_clip * sig
        act[src] = (gated * (up_clip + 1.0)).astype(BF16)
        slope = sig + GATE_SLOPE * gated * (1.0 - sig)
        gpg = jnp.where(gate_pre < CLAMP_LIMIT, act_grad * (up_clip + 1.0) * slope, 0.0)
        upg = jnp.where(jnp.abs(up_pre) < CLAMP_LIMIT, act_grad * gated, 0.0)
        both = jnp.concatenate([gpg, upg], axis=1).astype(BF16)
        gug[src] = both
        for t in range(n_tp):
            back[k, t % 2, t // 2] = dot(both, gu[pl.ds(t * q, q), :], 1, 1).astype(BF16)
        part_copy(k).start()

    def first(k):
        part_copy(k).wait_recv()
        xbuf[k] = (back[k, core, oplane].astype(F32) + part[k, oplane].astype(F32)).astype(BF16)
        x_copy(k).start()

    def second(k):
        x_copy(k).wait_recv()
        total = (
            back[k, core, plane].astype(F32) + part[k, plane].astype(F32) + xrecv[k].astype(F32)
        ).astype(BF16)

        @pl.when(k == 0)
        def _():
            ret[0] = total

        @pl.when(k > 0)
        def _():
            sendbuf[k] = total
            home_copy(k).start()

    def local_retention():
        for h in range(heads):
            score = fine(qrf[h], krf[h], 1, 1) * mask[h]
            wts[h] = score.astype(BF16)
            normed_f[:, h * vd : (h + 1) * vd] = fine(score, val[h], 1, 0)

    compute(0)
    local_retention()

    def step(n, carry):
        k = turn_of(n)

        @pl.when((n < n_sp) & (k < half_sp))
        def _():
            spot = full.at[peer(k), core]
            push(spot, spot, ssem.at[k], rsem.at[k], (me, far)).wait_recv()
            near_pair(k, core).start()

        @pl.when((n < n_sp) & (k >= half_sp))
        def _():
            spot = full.at[peer(k), core, plane]
            push(spot, spot, ssem.at[k], rsem.at[k], (me, far)).wait_recv()
            far_copy(k, plane).start()
            near_copy(k, core).start()

        j = turn_of(n - 1)

        @pl.when((n <= n_sp) & (j >= half_sp))
        def _():
            far_copy(j, oplane).wait_recv()
            relay_copy(j, core).start()

        @pl.when((n == past.slot * pace) & (past.slot > 0))
        def _():
            past.step(inner)

        @pl.when(n == pace)
        def _():
            lax.fori_loop(early, n_sp, send_rest, 0)

        @pl.when(n == 1)
        def _():
            first(0)

        @pl.when(n == 2)
        def _():
            second(0)

        @pl.when((n >= 3) & (n < n_sp + 2))
        def _():
            compute(turn_of(n - 2))

        @pl.when((n >= 4) & (n < n_sp + 3))
        def _():
            first(turn_of(n - 3))

        @pl.when((n >= 5) & (n < n_sp + 4))
        def _():
            second(turn_of(n - 4))

        return carry

    lax.fori_loop(1, n_sp + 4, step, 0)

    for j in range(heads * SPLIT):
        incoming[j // SPLIT, pl.ds((j % SPLIT) * rows_of, rows_of), :] = past.result(j)
    for h in range(heads):
        band = slice(h * vd, (h + 1) * vd)
        kept = normed_f[:, band] + dec[h] * fine(qrf[h], incoming[h], 1, 0)
        inverse = lax.rsqrt(jnp.mean(kept * kept, axis=1, keepdims=True) + EPSILON)
        inv[h] = inverse
        normed_f[:, band] = kept * inverse
        normed_own[:, band] = (kept * inverse).astype(BF16)
    normed_all[me] = normed_own[...]
    spread = Chain(normed_own, normed_all, n_sp, me, c, chain_sem, (0, 1))
    spread.start()

    def arrive(k, total):
        push(sendbuf.at[k], ret.at[k], hs.at[k], hr.at[k], (me, far)).wait_recv()
        return total + dot(pick[peer(k)], ret[k], 0, 0)

    total = og[:, cols(c)].astype(F32) + dot(pick[me], ret[0], 0, 0)
    total = lax.fori_loop(1, n_sp, arrive, total)
    half = tokens // 2
    resid[core, plane] = total.astype(BF16)

    def strip(side, p, i):
        return resid.at[side, p, pl.ds(i * half, half)]

    sent = []
    for i in range(2):
        mine = strip(core, plane, i)
        sent.append(push(mine, mine, gs.at[0, i], gr.at[0, i], (me, far)))
    for i in range(2):
        mine = strip(core, plane, i)
        sent.append(push(mine, mine, gs.at[1, i], gr.at[1, i], (me, near)))
    for cp in sent:
        cp.start()

    def share(side, p):
        return dot(resid[side, p], pw[cols(2 * p + side), :], 1, 0)

    normed_grad = share(core, plane)
    for i in range(2):
        spot = strip(core, oplane, i)
        push(spot, spot, gs.at[0, i], gr.at[0, i], (me, far)).wait_recv()
        onward = push(spot, spot, gs.at[2, i], gr.at[2, i], (me, near))
        onward.start()
        sent.append(onward)
    spread.step(1)
    normed_grad = normed_grad + share(core, oplane)
    for j, p in ((1, plane), (2, oplane)):
        for i in range(2):
            spot = strip(ocore, p, i)
            push(spot, spot, gs.at[j, i], gr.at[j, i], (me, near)).wait_recv()
        normed_grad = normed_grad + share(ocore, p)

    group = rcols.shape[3]
    per_quarter = q // group
    per_group = group * n_sp // (q * n_tp)

    strips = tokens // n_tp

    def band_of(index, strip_of):
        g = index // per_group
        quarter = g // per_quarter
        return resid.at[
            lax.rem(quarter, 2), quarter // 2,
            pl.ds(pl.multiple_of(strip_of * strips, 16), strips),
            pl.ds(pl.multiple_of(lax.rem(g, per_quarter) * group, 128), group),
        ]

    def col_copy(k):
        return push(
            band_of(peer(k), c), rcols.at[me, c], cs.at[k], cr.at[k], (peer(k), c)
        )

    def col_far(k, t):
        spot = rcols.at[peer(k), t]
        return push(spot, spot, as_.at[k], ar.at[k], (me, far))

    def col_near(k, t):
        spot = rcols.at[peer(k), t]
        return push(spot, spot, ds.at[k], dr.at[k], (me, near))

    def col_relay(k, t):
        spot = rcols.at[peer(k), t]
        return push(spot, spot, bs.at[k], br.at[k], (me, near))

    def send_cols(k, carry):
        col_copy(k).start()
        return carry

    def share_cols(k, carry):
        spot = rcols.at[peer(k), c]
        push(spot, spot, cs.at[k], cr.at[k], (me, far)).wait_recv()
        col_far(k, c).start()
        col_near(k, c).start()
        return carry

    def relay_cols(k, carry):
        col_far(k, far).wait_recv()
        col_relay(k, far).start()
        return carry

    def wait_cols(k, carry):
        col_near(k, near).wait_recv()
        col_relay(k, near_far).wait_recv()
        return carry

    grads = []
    for h in range(heads):
        band = slice(h * vd, (h + 1) * vd)
        ng = normed_grad[:, band]
        nf = normed_f[:, band]
        grad = inv[h] * (ng - nf * jnp.mean(ng * nf, axis=1, keepdims=True))
        grad_f[h] = grad
        grad_bf = grad.astype(BF16)
        grads.append(grad_bf)
        turned = (qrf[h] * dec[h]).astype(BF16)
        state = dot(turned, grad_bf, 0, 0)
        for s in range(SPLIT):
            inner_g[h * SPLIT + s] = state[s * rows_of : (s + 1) * rows_of]

    def weights_grad(t):
        x = flat(full[:, lax.rem(t, 2), t // 2, 0])
        g = flat(full[:, lax.rem(t, 2), t // 2, 1])
        both = dot(x, flat(gug[...]), 0, 0).astype(BF16)
        gate_o[0, cols(t), :] = both[:, :hid]
        up_o[0, cols(t), :] = both[:, hid:]
        down_o[0, :, cols(t)] = dot(flat(act[...]), g, 0, 0).astype(BF16)

    @pl.when(coming.slot == 0)
    def _():
        coming.step(inner_g)

    lax.fori_loop(1, n_sp, send_cols, 0)
    for t in range(n_tp):
        rcols[me, t] = band_of(me, t)[...]
    last = max(pairs, n_tp) - 1

    def late(s, carry):
        for d in range(2, pairs):

            @pl.when(s == d - 1)
            def _():
                spread.step(d)

        @pl.when(s == last)
        def _():
            lax.fori_loop(1, n_sp, share_cols, 0)

        @pl.when((s > 0) & (s < n_tp))
        def _():
            weights_grad(s)

        @pl.when(s == last)
        def _():
            lax.fori_loop(1, n_sp, relay_cols, 0)

        @pl.when((s == coming.slot) & (s > 0))
        def _():
            coming.step(inner_g)

        return carry

    lax.fori_loop(1, last + 1, late, 0)
    weights_grad(0)

    def unturn(x):
        return x * cosb[...] - swapped(x) * sinb[...]

    partial = []
    for h in range(heads):
        score = (fine(grad_f[h], val[h], 1, 1) * mask[h]).astype(BF16)
        qp = dot(score, kr[h], 1, 0) + dec[h] * fine(grad_f[h], incoming[h], 1, 1)
        query_o[:, h * kd : (h + 1) * kd] = unturn(qp).astype(BF16)
        partial.append((dot(score, qr[h], 0, 0), dot(wts[h], grads[h], 0, 0)))

    lax.fori_loop(1, n_sp, wait_cols, 0)
    spread.finish()
    columns = rcols[...].reshape(n_sp * tokens, group)
    everyone = normed_all[...].reshape(n_sp * tokens, heads * vd)
    proj[...] = dot(columns, everyone, 0, 0)
    width = proj_o.shape[0]
    proj_o[...] = proj[pl.ds(pl.multiple_of(lax.rem(me, per_group) * width, 8), width), :]

    future = [coming.result(j) for j in range(heads * SPLIT)]
    for h in range(heads):
        band = slice(h * vd, (h + 1) * vd)
        key_part, value_part = partial[h]
        later = jnp.concatenate(future[h * SPLIT : (h + 1) * SPLIT], axis=0)
        kp = key_part + rem_[h] * dot(val[h], later, 1, 1)
        key_o[:, h * kd : (h + 1) * kd] = (unturn(kp) * scale).astype(BF16)
        value_o[:, band] = (value_part + rem_[h] * dot(kr[h], later, 1, 0)).astype(BF16)

    for cp in sent:
        cp.wait_send()
    past.finish()
    coming.finish()

    def drain(k, carry):
        part_copy(k).wait_send()
        x_copy(k).wait_send()

        @pl.when(k < half_sp)
        def _():
            near_pair(k, core).wait_send()

        @pl.when((k > 0) & (k < half_sp))
        def _():
            out_pair(k).wait_send()

        @pl.when(k >= half_sp)
        def _():
            out_copy(k).wait_send()
            far_copy(k, plane).wait_send()
            near_copy(k, core).wait_send()
            relay_copy(k, core).wait_send()

        @pl.when(k > 0)
        def _():
            home_copy(k).wait_send()
            col_copy(k).wait_send()
            col_far(k, c).wait_send()
            col_near(k, c).wait_send()
            col_relay(k, far).wait_send()

        return carry

    lax.fori_loop(0, n_sp, drain, 0)


def finish_kernel(
    gate, up, down, proj, query, key, value, gate_o, up_o, down_o, proj_o, query_o, key_o, value_o,
    sem,
):
    pairs = ((gate, gate_o), (up, up_o), (down, down_o), (proj, proj_o))
    stores = [pltpu.make_async_copy(a, b, sem.at[i]) for i, (a, b) in enumerate(pairs)]
    for cp in stores:
        cp.start()
    for a, b in ((query, query_o), (key, key_o), (value, value_o)):
        width = b.shape[2]
        for h in range(b.shape[1]):
            b[:, h, :] = a[:, h * width : (h + 1) * width]
    for cp in stores:
        cp.wait()


def rotation_tables(n_sp, tokens, key_width):
    frequency = 10000.0 ** -np.linspace(0.0, 1.0, key_width // 2)
    frequency = np.repeat(frequency, 2)
    angle = np.arange(tokens)[:, None] * frequency[None, :]
    start = tokens * np.arange(n_sp)[:, None] * frequency[None, :]
    return [
        jnp.asarray(table.astype(np.float32))
        for table in (np.cos(angle), np.sin(angle), np.cos(start), np.sin(start))
    ]


def per_device(
    stream, out_grad, routes, route_weight, queries, key_vectors, value_vectors, log_decay,
    out_proj, gate_weight, up_weight, down_weight,
):
    n_sp = lax.axis_size("sp")
    n_tp = lax.axis_size("tp")
    tokens, width = stream.shape
    cap = 4 * tokens // n_sp
    q = width // n_tp
    heads, kd = queries.shape[1:]
    vd = value_vectors.shape[2]
    hid = gate_weight.shape[2]
    w = width // n_sp
    group = max(w, 128)
    count, rows_of = heads * SPLIT, kd // SPLIT
    vmem, dma = pltpu.VMEM, pltpu.SemaphoreType.DMA
    block = vmem((n_sp, cap, q), BF16)
    packet = vmem((count, rows_of, vd), BF16)
    tables = rotation_tables(n_sp, tokens, kd)
    outs = pl.pallas_call(
        functools.partial(whole_kernel, n_sp, n_tp, heads),
        out_shape=(
            vmem(gate_weight.shape, BF16),
            vmem(up_weight.shape, BF16),
            vmem(down_weight.shape, BF16),
            vmem((w, heads * vd), F32),
            vmem((tokens, heads * kd), BF16),
            vmem((tokens, heads * kd), BF16),
            vmem((tokens, heads * vd), BF16),
        ),
        in_specs=vmem_specs(12) + [pl.BlockSpec(memory_space=pltpu.HBM)] * 4,
        out_specs=tuple(vmem_specs(7)),
        scratch_shapes=[
            vmem((n_sp, 2, 2, 2, cap, q), BF16),
            vmem((n_sp, 2, 2, cap, q), BF16),
            vmem((width, 2 * hid), BF16),
            vmem((hid, width), BF16),
            vmem((width, heads * vd), BF16),
            vmem((n_sp, cap, hid), BF16),
            vmem((n_sp, cap, 2 * hid), BF16),
            vmem((n_sp, 2, 2, cap, q), BF16),
            vmem((n_sp, 2, cap, q), BF16),
            block, block, block, block,
            vmem((n_sp, cap, tokens), BF16),
            vmem((n_sp, cap, 1), F32),
            vmem((n_sp, tokens), F32),
            vmem((n_sp, tokens), F32),
            vmem((2, 2, tokens, q), BF16),
            vmem((n_sp, n_tp, tokens // n_tp, group), BF16),
            vmem((tokens, heads * vd), BF16),
            vmem((n_sp, tokens, heads * vd), BF16),
            vmem((tokens, heads * vd), F32),
            vmem((heads, tokens, 1), F32),
            vmem((heads, tokens, 1), F32),
            vmem((heads, tokens, 1), F32),
            vmem((heads, tokens, tokens), F32),
            vmem((heads, tokens, tokens), BF16),
            vmem((heads, tokens, kd), BF16),
            vmem((heads, tokens, kd), BF16),
            vmem((heads, tokens, kd), F32),
            vmem((heads, tokens, kd), F32),
            vmem((heads, tokens, vd), F32),
            vmem((heads, tokens, vd), BF16),
            vmem((tokens, kd), F32),
            vmem((tokens, kd), F32),
            vmem((heads, 8, 128), F32),
            vmem((heads, 8, 128), F32),
            vmem((count, rows_of, vd), F32),
            vmem((count, rows_of, vd), F32),
            vmem((heads, kd, vd), BF16),
            vmem((group, heads * vd), F32),
        ]
        + [packet] * 8
        + [dma((4,)), dma((2,))]
        + [dma((n_sp,))] * 14
        + [dma((3, 2))] * 2
        + [dma((n_sp,))] * 8
        + [dma((count,))] * 8
        + [dma((2, n_sp // 2))] * 4,
        compiler_params=pltpu.CompilerParams(
            collective_id=0, has_side_effects=True, vmem_limit_bytes=58 * 2**20
        ),
        name="whole",
    )(
        stream, out_grad, routes.T, route_weight.T, queries, key_vectors, value_vectors,
        log_decay.T, *tables, gate_weight, up_weight, down_weight, out_proj,
    )
    shapes = [jax.ShapeDtypeStruct(x.shape, x.dtype) for x in outs[:4]] + [
        jax.ShapeDtypeStruct(x.shape, BF16) for x in (queries, key_vectors, value_vectors)
    ]
    return pl.pallas_call(
        finish_kernel,
        out_shape=tuple(shapes),
        in_specs=vmem_specs(7),
        out_specs=tuple(any_specs(4) + vmem_specs(3)),
        scratch_shapes=[dma((4,))],
        compiler_params=pltpu.CompilerParams(vmem_limit_bytes=16 * 2**20),
        name="finish",
    )(*outs)


def solution(mesh):
    in_specs = (
        P("sp", None),
        P("sp", None),
        P("sp", None),
        P("sp", None),
        P("sp", "tp", None),
        P("sp", "tp", None),
        P("sp", "tp", None),
        P("sp", "tp"),
        P(None, "tp"),
        P("sp", None, "tp"),
        P("sp", None, "tp"),
        P("sp", "tp", None),
    )
    out_specs = (
        P("sp", None, "tp"),
        P("sp", None, "tp"),
        P("sp", "tp", None),
        P("sp", "tp"),
        P("sp", "tp", None),
        P("sp", "tp", None),
        P("sp", "tp", None),
    )
    return jax.shard_map(
        per_device, mesh=mesh, in_specs=in_specs, out_specs=out_specs, check_vma=False
    )
```
